32 devices in a mesh: sp: 8 (over z, x), tp: 4 (over y, core).
Axes of the slice: x: 2, y: 2, z: 4, core: 2. Of those that a mesh axis runs over, the one named last changes fastest.
Arguments:
- tokens: bfloat16 [8192, 2048], P('sp', 'tp'), may hold values from -70 to 70
- w_query: bfloat16 [2048, 1024], P(None, 'tp'), may hold values from -0.125 to 0.125
- w_key: bfloat16 [2048, 1024], P(None, 'tp'), may hold values from -0.125 to 0.125
- w_value: bfloat16 [2048, 1024], P(None, 'tp'), may hold values from -0.125 to 0.125
- w_delta_gate: bfloat16 [2048, 1024], P(None, 'tp'), may hold values from -0.125 to 0.125
- w_glu_value: bfloat16 [2048, 1024], P(None, 'tp'), may hold values from -0.125 to 0.125
- w_glu_gate: bfloat16 [2048, 1024], P(None, 'tp'), may hold values from -0.125 to 0.125
- w_conv_gate: bfloat16 [2048, 1024], P(None, 'tp'), may hold values from -0.125 to 0.125
- w_beta: bfloat16 [2048, 8], replicated, may hold values from -0.125 to 0.125
- w_decay: bfloat16 [2048, 8], replicated, may hold values from -0.125 to 0.125
- decay_log: float32 [8], replicated, may hold values from -12 to -3
- head_gain: float32 [128], replicated, may hold values from 0.1 to 1.9
- conv_taps: bfloat16 [31, 1024], P(None, 'tp'), may hold values from -2.5 to 2.5
- ln_gain: float32 [1024], P('tp'), may hold values from 0.1 to 1.9
- ln_shift: float32 [1024], P('tp'), may hold values from -3 to 3
- out_delta: bfloat16 [1024, 2048], P('tp'), may hold values from -0.125 to 0.125
- out_conv: bfloat16 [1024, 2048], P('tp'), may hold values from -0.125 to 0.125
Outputs:
- mixed_out: bfloat16 [8192, 2048], P(('sp', 'tp'))
The draws below stay inside these ranges and needn't reach their ends.
All inputs are finite; a program needn't handle non-finite values.
Results may differ from the reference program's by a relative error of at most 0.024.
Values may be sent and summed in bfloat16 or wider, within the bound.
A program may use at most 64 MiB of HBM per device.

```python
import jax
import jax.numpy as jnp
from jax import lax

D = 2048
HEADS = 8
DK = 128
CV = 1024
KERNEL = 31
SPAN = 64
TOKENS = 8192
N_TP = 4


def draw_tokens(key, part):
    keys = jax.random.split(key, 3)
    span_rows = 4 * SPAN
    groups = (TOKENS + span_rows - 1) // span_rows
    shifts = jnp.clip(jax.random.normal(keys[1], (groups, D), jnp.float32), -6.0, 6.0) * 1.5
    shifts = jnp.repeat(shifts, span_rows, axis=0)[:TOKENS]
    noise = jnp.clip(jax.random.normal(keys[0], (TOKENS, D), jnp.float32), -6.0, 6.0)
    spread = 0.7
    scales = jnp.exp(jax.random.uniform(keys[2], (TOKENS, 1), jnp.float32, -spread, spread))
    return ((noise + shifts) * scales).astype(jnp.bfloat16)


def draw_decay_log(key, part):
    keys = jax.random.split(key, 3)
    order = jax.random.permutation(keys[0], HEADS)
    fast_heads = HEADS // 2
    slow_rate = jax.random.uniform(keys[1], (HEADS,), jnp.float32, 0.3, 1.0) * 2.3 / TOKENS
    fast_rate = jax.random.uniform(keys[2], (HEADS,), jnp.float32, 0.015, 0.04)
    return jnp.log(jnp.where(order < fast_heads, fast_rate, slow_rate)).astype(jnp.float32)


def draw_conv_taps(key, part):
    keys = jax.random.split(key, 2)
    noise = jnp.clip(jax.random.normal(keys[0], (KERNEL, CV), jnp.float32), -4.0, 4.0)
    spread = 1.2
    levels = jnp.exp(jax.random.uniform(keys[1], (16,), jnp.float32, -spread, spread))
    group_ids = jnp.arange(CV) * 16 // CV
    column_scale = jnp.take(levels, group_ids)
    return (noise * column_scale[None, :] * KERNEL ** (-0.5)).astype(jnp.bfloat16)


def level_of(key, shape, shards, smallest, high):
    def one(axis_at, shards_of):
        heights = jax.random.uniform(jax.random.fold_in(jax.random.fold_in(key, 6), axis_at), (shards_of,), jnp.float32, smallest / len(shards), high / len(shards))
        return jnp.repeat(jnp.exp(heights), shape[axis_at] // shards_of).reshape((-1,) + (1,) * (len(shape) - axis_at - 1))

    loudness = one(*shards[0])
    for cut in shards[1:]:
        loudness = loudness * one(*cut)
    return loudness


def gaussian(own_key, shape, scale, reach, shards=(), kind=jnp.bfloat16):
    entries = scale * jax.random.normal(own_key, shape, jnp.float32)
    if shards:
        entries = entries * level_of(own_key, shape, shards, -0.22, 0.18)
    return jnp.clip(entries, -reach, reach).astype(kind)


def setup_inputs(seed: int = 0) -> dict:
    splits = jax.random.split(jax.random.key(seed), 18)
    tokens = draw_tokens(jax.random.fold_in(splits[17], 71), 0)
    w_query = gaussian(splits[1], (D, HEADS * DK), D ** -0.5, 0.125, ((1, 4),))
    w_key = gaussian(splits[2], (D, HEADS * DK), D ** -0.5, 0.125, ((1, 4),))
    w_value = gaussian(splits[3], (D, HEADS * DK), D ** -0.5, 0.125, ((1, 4),))
    w_delta_gate = gaussian(splits[4], (D, HEADS * DK), D ** -0.5, 0.125, ((1, 4),))
    w_glu_value = gaussian(splits[5], (D, CV), D ** -0.5, 0.125, ((1, 4),))
    w_glu_gate = gaussian(splits[6], (D, CV), D ** -0.5, 0.125, ((1, 4),))
    w_conv_gate = gaussian(splits[7], (D, CV), D ** -0.5, 0.125, ((1, 4),))
    w_beta = gaussian(splits[8], (D, HEADS), D ** -0.5, 0.125)
    w_decay = gaussian(splits[9], (D, HEADS), D ** -0.5, 0.125)
    decay_log = draw_decay_log(jax.random.fold_in(splits[17], 71), 0)
    head_gain = jnp.clip(1.0 + 0.18 * jax.random.normal(splits[11], (DK,), jnp.float32), 0.1, 1.9)
    conv_taps = draw_conv_taps(jax.random.fold_in(splits[17], 71), 0)
    ln_gain = jnp.clip(1.0 + 0.18 * jax.random.normal(splits[13], (CV,), jnp.float32), 0.1, 1.9)
    ln_shift = gaussian(splits[14], (CV,), 0.5, 3.0, ((0, 4),), jnp.float32)
    out_delta = gaussian(splits[15], (HEADS * DK, D), (HEADS * DK + CV) ** -0.5, 0.125, ((0, 4),))
    out_conv = gaussian(splits[16], (CV, D), (HEADS * DK + CV) ** -0.5, 0.125, ((0, 4),))
    return {"tokens": tokens, "w_query": w_query, "w_key": w_key, "w_value": w_value, "w_delta_gate": w_delta_gate, "w_glu_value": w_glu_value, "w_glu_gate": w_glu_gate, "w_conv_gate": w_conv_gate, "w_beta": w_beta, "w_decay": w_decay, "decay_log": decay_log, "head_gain": head_gain, "conv_taps": conv_taps, "ln_gain": ln_gain, "ln_shift": ln_shift, "out_delta": out_delta, "out_conv": out_conv}


TINY_NORM = 1e-06
TINY_VAR = 1e-05
HIGHEST = lax.Precision.HIGHEST

def head_rule(query, keys, values, strength, log_decay):
    blocks = query.shape[0] // SPAN

    def split_blocks(array):
        return array.reshape((blocks, SPAN) + array.shape[1:])
    query, keys, values = (split_blocks(query), split_blocks(keys), split_blocks(values))
    strength, log_decay = (split_blocks(strength), split_blocks(log_decay))
    log_sum = jnp.cumsum(log_decay, axis=-1)
    offsets = jnp.arange(SPAN)
    causal = offsets[:, None] >= offsets[None, :]
    strict = offsets[:, None] > offsets[None, :]
    spread = log_sum[:, :, None] - log_sum[:, None, :]
    damping = jnp.where(causal, jnp.exp(jnp.where(causal, spread, 0.0)), 0.0)
    scaled_keys = keys * strength[..., None]
    lower = jnp.where(strict, jnp.einsum('nid,njd->nij', scaled_keys, keys, precision=HIGHEST) * damping, 0.0)
    identity = jnp.eye(SPAN, dtype=jnp.float32)
    right = jnp.concatenate([values * strength[..., None], scaled_keys * jnp.exp(log_sum)[..., None]], axis=-1)
    solved = jax.scipy.linalg.solve_triangular(identity + lower, right, lower=True, unit_diagonal=True)
    width = values.shape[-1]
    corrected = solved[..., :width]
    key_terms = solved[..., width:]
    scores = jnp.einsum('nid,njd->nij', query, keys, precision=HIGHEST) * damping

    def advance(memory, inputs):
        query_block, keys_block, corrected_block, terms_block, scores_block, log_block = inputs
        fresh = corrected_block - jnp.dot(terms_block, memory, precision=HIGHEST)
        output = jnp.dot(query_block * jnp.exp(log_block)[:, None], memory, precision=HIGHEST)
        output = output + jnp.dot(scores_block, fresh, precision=HIGHEST)
        tail_log = log_block[-1]
        weighted = keys_block * jnp.exp(tail_log - log_block)[:, None]
        memory = memory * jnp.exp(tail_log) + jnp.dot(weighted.T, fresh, precision=HIGHEST)
        return (memory, output)
    start = jnp.zeros((keys.shape[-1], width), jnp.float32)
    ignored, outputs = lax.scan(advance, start, (query, keys, corrected, key_terms, scores, log_sum))
    return outputs.reshape(blocks * SPAN, width)

def reference(tokens, w_query, w_key, w_value, w_delta_gate, w_glu_value, w_glu_gate, w_conv_gate, w_beta, w_decay, decay_log, head_gain, conv_taps, ln_gain, ln_shift, out_delta, out_conv):
    length = tokens.shape[0]
    floats = tokens.astype(jnp.float32)
    inv_rms = lax.rsqrt(lax.optimization_barrier(jnp.mean(floats * floats, axis=1, keepdims=True)) + TINY_NORM)

    def project(weight):
        return jnp.dot(tokens.astype(jnp.float32), weight.astype(jnp.float32), preferred_element_type=jnp.float32) * inv_rms
    query_raw = project(w_query).astype(jnp.bfloat16)
    key_raw = project(w_key).astype(jnp.bfloat16)
    value_raw = project(w_value).astype(jnp.bfloat16)
    delta_gate_raw = project(w_delta_gate).astype(jnp.bfloat16)
    glu_value_raw = project(w_glu_value).astype(jnp.bfloat16)
    glu_gate_raw = project(w_glu_gate).astype(jnp.bfloat16)
    conv_gate_raw = project(w_conv_gate).astype(jnp.bfloat16)
    strength = jax.nn.sigmoid(project(w_beta))
    log_decay = -jnp.exp(decay_log)[None, :] * jax.nn.softplus(project(w_decay))

    def to_heads(raw):
        return raw.astype(jnp.float32).reshape(length, HEADS, DK)

    def unit_rows(array):
        return array * lax.rsqrt(lax.optimization_barrier(jnp.sum(array * array, axis=-1, keepdims=True)) + TINY_NORM)
    query = unit_rows(to_heads(query_raw)) * DK ** (-0.5)
    keys = unit_rows(to_heads(key_raw))
    values = to_heads(value_raw)
    heads_out = lax.map(lambda inputs: head_rule(*inputs), (jnp.moveaxis(query, 1, 0), jnp.moveaxis(keys, 1, 0), jnp.moveaxis(values, 1, 0), strength.T, log_decay.T))
    output = jnp.moveaxis(heads_out, 0, 1)
    output = output * lax.rsqrt(lax.optimization_barrier(jnp.mean(output * output, axis=-1, keepdims=True)) + TINY_NORM) * head_gain
    delta_mixed = (output.reshape(length, HEADS * DK) * jax.nn.silu(delta_gate_raw.astype(jnp.float32))).astype(jnp.bfloat16)
    gated_units = (glu_value_raw.astype(jnp.float32) * jax.nn.sigmoid(glu_gate_raw.astype(jnp.float32))).astype(jnp.bfloat16)
    padded = jnp.concatenate([jnp.zeros((KERNEL - 1, CV), jnp.bfloat16), gated_units], axis=0)
    filtered = jnp.zeros((length, CV), jnp.float32)
    for offset in range(KERNEL):
        filtered = filtered + padded[offset:offset + length].astype(jnp.float32) * conv_taps[offset].astype(jnp.float32)
    center = lax.optimization_barrier(jnp.sum(filtered, axis=1)) / CV
    variance = jnp.maximum(lax.optimization_barrier(jnp.sum(filtered * filtered, axis=1)) / CV - center * center, 0.0)
    normed = (filtered - center[:, None]) * lax.rsqrt(variance + TINY_VAR)[:, None] * ln_gain + ln_shift
    conv_mixed = (jax.nn.silu(normed) * jax.nn.silu(conv_gate_raw.astype(jnp.float32))).astype(jnp.bfloat16)
    head_block = HEADS * DK // N_TP
    chan_block = CV // N_TP
    summed = jnp.zeros((length, D), jnp.float32)
    for group in range(N_TP):
        partial_value = jnp.dot(delta_mixed[:, group * head_block:(group + 1) * head_block].astype(jnp.float32), out_delta[group * head_block:(group + 1) * head_block].astype(jnp.float32), preferred_element_type=jnp.float32)
        partial_value = partial_value + jnp.dot(conv_mixed[:, group * chan_block:(group + 1) * chan_block].astype(jnp.float32), out_conv[group * chan_block:(group + 1) * chan_block].astype(jnp.float32), preferred_element_type=jnp.float32)
        partial_value = lax.optimization_barrier(partial_value.astype(jnp.bfloat16))
        summed = summed + partial_value.astype(jnp.float32)
    return summed.astype(jnp.bfloat16)
```

```python
import functools

import jax
import jax.numpy as jnp
from jax import lax
from jax.experimental import pallas as pl
from jax.experimental.pallas import tpu as pltpu
from jax.sharding import PartitionSpec as P

BLOCK = 128


TINY_NORM = 1e-06
TINY_VAR = 1e-05
HIGHEST = lax.Precision.HIGHEST


def shifted(block, axis, distance):
    devices = range(lax.axis_size(axis))
    route = [(i - distance, i) for i in devices if i - distance in devices]
    return lax.ppermute(block, axis, route)


def nt(a, b):
    return lax.dot_general(a, b, (((1,), (1,)), ((), ())), preferred_element_type=jnp.float32)


def mm(a, b):
    return jnp.dot(
        a.astype(jnp.bfloat16), b.astype(jnp.bfloat16), preferred_element_type=jnp.float32
    )


def delta_kernel(
    heads, width, q_ref, k_ref, v_ref, g_ref, outa_ref, outb_ref, state_ref,
    lhs_s, corr_s, score_s, wt_s, tail_s,
):
    rows = q_ref.shape[0]
    blocks = rows // BLOCK
    row_id = lax.broadcasted_iota(jnp.int32, (BLOCK, BLOCK), 0)
    col_id = lax.broadcasted_iota(jnp.int32, (BLOCK, BLOCK), 1)
    causal = row_id >= col_id
    strict = row_id > col_id
    differ = row_id ^ col_id
    eye = jnp.where(row_id == col_id, 1.0, 0.0)
    tril = jnp.where(causal, 1.0, 0.0)

    def prepare(c):
        at = pl.ds(pl.multiple_of(c * BLOCK, BLOCK), BLOCK)
        gates = g_ref[at, :]
        sums = jnp.dot(tril, gates, precision=HIGHEST, preferred_element_type=jnp.float32)
        chains = []
        for h in range(heads):
            lanes = slice(h * width, (h + 1) * width)
            k, q = k_ref[at, lanes], q_ref[at, lanes]
            v = v_ref[at, lanes].astype(jnp.float32)
            kf, qf = k.astype(jnp.float32), q.astype(jnp.float32)
            ik = lax.rsqrt(jnp.sum(kf * kf, axis=-1, keepdims=True) + TINY_NORM)
            iq = lax.rsqrt(jnp.sum(qf * qf, axis=-1, keepdims=True) + TINY_NORM)
            iq = iq * width ** (-0.5)
            beta = gates[:, h : h + 1]
            log_sum = sums[:, heads + h : heads + h + 1]
            log_full = jnp.broadcast_to(log_sum, (BLOCK, BLOCK))
            spread = log_full - log_full.T
            damp = jnp.where(causal, jnp.exp(jnp.where(causal, spread, 0.0)), 0.0)
            damp = damp * jnp.broadcast_to(ik, (BLOCK, BLOCK)).T
            lower = jnp.where(strict, nt(k, k) * damp * (beta * ik), 0.0)
            score_s[h, at, :] = (nt(q, k) * damp * iq).astype(jnp.bfloat16)
            grow = jnp.exp(log_sum)
            right = jnp.concatenate([v * beta, kf * (beta * ik * grow)], axis=1)
            tail = log_full[BLOCK - 1 : BLOCK, :]
            weighted = kf * (ik * jnp.exp(tail[:, :1] - log_sum))
            wt_s[h, c] = weighted.T.astype(jnp.bfloat16)
            tail_s[h, c] = jnp.broadcast_to(jnp.exp(tail), (8, BLOCK))
            lhs_s[h, c, BLOCK:, :] = (qf * (iq * grow)).astype(jnp.bfloat16)
            chains.append([h, lower, right, eye - jnp.where(differ == 1, lower, 0.0)])
        return at, c, chains

    def pair(p, carry):
        prepared = [prepare(p * 2 + i) for i in range(2)]
        size = 2
        while size < BLOCK:
            level = (differ >= size) & (differ < 2 * size)
            parts = [
                [mm(jnp.where(level, ch[1], 0.0), ch[3]) for ch in item[2]] for item in prepared
            ]
            for item, part in zip(prepared, parts):
                for ch, moved in zip(item[2], part):
                    ch[3] = ch[3] - mm(ch[3], moved)
            size *= 2
        for at, c, chains in prepared:
            for h, lower, right, inverse in chains:
                solved = mm(inverse, right)
                corr_s[h, at, :] = solved[:, :width]
                lhs_s[h, c, :BLOCK, :] = solved[:, width:].astype(jnp.bfloat16)
        return carry

    lax.fori_loop(0, blocks // 2, pair, 0)
    for h in range(heads):
        state_ref[h] = jnp.concatenate([eye, jnp.zeros((width, width), jnp.float32)], axis=1)

    def advance(c, carry):
        at = pl.ds(pl.multiple_of(c * BLOCK, BLOCK), BLOCK)
        boths = [mm(lhs_s[h, c], state_ref[h]) for h in range(heads)]
        fresh = []
        for h in range(heads):
            first = boths[h][:BLOCK]
            fresh.append(
                jnp.concatenate(
                    [-first[:, :width], corr_s[h, at, :] - first[:, width:]], axis=1
                ).astype(jnp.bfloat16)
            )
        for h in range(heads):
            decay = tail_s[h, c][:1, :]
            decay = jnp.concatenate([decay, decay], axis=1)
            state_ref[h] = state_ref[h] * decay + mm(wt_s[h, c], fresh[h])
        for h in range(heads):
            out = boths[h][BLOCK:] + mm(score_s[h, at, :], fresh[h])
            outa_ref[h, at, :] = out[:, :width].astype(jnp.bfloat16)
            outb_ref[h, at, :] = out[:, width:]
        return carry

    lax.fori_loop(0, blocks, advance, 0)


def delta_rule(query_raw, key_raw, value_raw, gates, heads, width):
    rows = query_raw.shape[0]
    blocks = rows // BLOCK
    vm = pl.BlockSpec(memory_space=pltpu.VMEM)
    return pl.pallas_call(
        functools.partial(delta_kernel, heads, width),
        out_shape=(
            jax.ShapeDtypeStruct((heads, rows, width), jnp.bfloat16),
            jax.ShapeDtypeStruct((heads, rows, width), jnp.float32),
            jax.ShapeDtypeStruct((heads, width, 2 * width), jnp.float32),
        ),
        in_specs=[vm] * 4,
        out_specs=(vm, vm, vm),
        scratch_shapes=[
            pltpu.VMEM((heads, blocks, 2 * BLOCK, width), jnp.bfloat16),
            pltpu.VMEM((heads, rows, width), jnp.float32),
            pltpu.VMEM((heads, rows, BLOCK), jnp.bfloat16),
            pltpu.VMEM((heads, blocks, width, BLOCK), jnp.bfloat16),
            pltpu.VMEM((heads, blocks, 8, BLOCK), jnp.float32),
        ],
        compiler_params=pltpu.CompilerParams(
            vmem_limit_bytes=40 * 1024 * 1024
        ),
        cost_estimate=pl.CostEstimate(
            flops=10_000_000_000, bytes_accessed=4_000_000, transcendentals=0
        ),
        name="delta_rule",
    )(query_raw, key_raw, value_raw, gates)


def finish_kernel(
    heads, width, place_ref, all_ref, outa_ref, outb_ref, gate_ref, gain_ref, mixed_ref, carry_s
):
    rows = outb_ref.shape[1]
    carry_s[...] = jnp.zeros_like(carry_s)

    def hop(i, carry):
        moved = [
            jnp.dot(
                all_ref[i, h, :, :width],
                carry_s[h],
                precision=HIGHEST,
                preferred_element_type=jnp.float32,
            )
            for h in range(heads)
        ]
        for h in range(heads):
            carry_s[h] = moved[h] + all_ref[i, h, :, width:]
        return carry

    lax.fori_loop(0, place_ref[0], hop, 0)
    tile = 256

    def one(c, carry):
        at = pl.ds(pl.multiple_of(c * tile, tile), tile)
        for h in range(heads):
            lanes = slice(h * width, (h + 1) * width)
            result = outb_ref[h, at, :] + mm(outa_ref[h, at, :], carry_s[h])
            result = result * lax.rsqrt(
                jnp.mean(result * result, axis=-1, keepdims=True) + TINY_NORM
            )
            gate = gate_ref[at, lanes].astype(jnp.float32)
            mixed_ref[at, lanes] = (result * gain_ref[...] * jax.nn.silu(gate)).astype(
                jnp.bfloat16
            )
        return carry

    lax.fori_loop(0, rows // tile, one, 0)


def finish(place, states, outa, outb, gate, gain, heads, width):
    rows = outb.shape[1]
    vm = pl.BlockSpec(memory_space=pltpu.VMEM)
    return pl.pallas_call(
        functools.partial(finish_kernel, heads, width),
        out_shape=jax.ShapeDtypeStruct((rows, heads * width), jnp.bfloat16),
        in_specs=[pl.BlockSpec(memory_space=pltpu.SMEM)] + [vm] * 5,
        out_specs=vm,
        scratch_shapes=[pltpu.VMEM((heads, width, width), jnp.float32)],
        compiler_params=pltpu.CompilerParams(vmem_limit_bytes=40 * 1024 * 1024),
        cost_estimate=pl.CostEstimate(
            flops=2_000_000_000, bytes_accessed=6_000_000, transcendentals=0
        ),
        name="delta_finish",
    )(place, states, outa, outb, gate, gain)


def local(
    tokens,
    w_query,
    w_key,
    w_value,
    w_delta_gate,
    w_glu_value,
    w_glu_gate,
    w_conv_gate,
    w_beta,
    w_decay,
    decay_log,
    head_gain,
    conv_taps,
    ln_gain,
    ln_shift,
    out_delta,
    out_conv,
):
    rows_here = tokens.shape[0]
    tp_size = lax.axis_size("tp")
    width_all = tokens.shape[1] * tp_size
    weights = (
        w_query,
        w_key,
        w_value,
        w_delta_gate,
        w_glu_value,
        w_glu_gate,
        w_conv_gate,
        w_beta,
        w_decay,
    )
    piece = lax.all_gather(tokens, "tp", axis=1, tiled=True)
    totals = tuple(
        (jnp.dot(piece, weight, preferred_element_type=jnp.float32) for weight in weights)
    )
    squares = jnp.sum(jnp.square(piece.astype(jnp.float32)), axis=1)
    sums, squares = (totals, squares)
    inv_rms = lax.rsqrt(squares / width_all + TINY_NORM)[:, None]
    scaled = [summed * inv_rms for summed in sums]
    query_raw, key_raw, value_raw, delta_gate_raw, glu_value_raw, glu_gate_raw, conv_gate_raw = [
        item.astype(jnp.bfloat16) for item in scaled[:7]
    ]
    head_size = head_gain.shape[0]
    heads_here = w_query.shape[1] // head_size
    first_head = lax.axis_index("tp") * heads_here
    strength = jax.nn.sigmoid(lax.dynamic_slice_in_dim(scaled[7], first_head, heads_here, 1))
    rates = jnp.exp(lax.dynamic_slice_in_dim(decay_log, first_head, heads_here, 0))
    log_decay = -rates[None, :] * jax.nn.softplus(
        lax.dynamic_slice_in_dim(scaled[8], first_head, heads_here, 1)
    )
    gates = jnp.concatenate(
        [
            strength,
            log_decay,
            jnp.zeros((rows_here, head_size - 2 * heads_here), jnp.float32),
        ],
        axis=1,
    )
    outa, outb, final = delta_rule(
        query_raw, key_raw, value_raw, gates, heads_here, head_size
    )
    states = lax.all_gather(final, "sp")
    place = lax.axis_index("sp").astype(jnp.int32).reshape(1)
    delta_mixed = finish(
        place, states, outa, outb, delta_gate_raw, head_gain[None, :], heads_here, head_size
    )
    kernel = conv_taps.shape[0]
    channels = conv_taps.shape[1]
    gated_units = (
        glu_value_raw.astype(jnp.float32) * jax.nn.sigmoid(glu_gate_raw.astype(jnp.float32))
    ).astype(jnp.bfloat16)
    before = shifted(gated_units[rows_here - (kernel - 1) :], "sp", 1)
    padded = jnp.concatenate([before, gated_units], axis=0)
    filtered = jnp.zeros((rows_here, channels), jnp.float32)
    for offset in range(kernel):
        filtered = filtered + padded[offset : offset + rows_here].astype(jnp.float32) * conv_taps[
            offset
        ].astype(jnp.float32)
    first_sum = jnp.sum(filtered, axis=1)
    second_sum = jnp.sum(filtered * filtered, axis=1)
    first_sum, second_sum = lax.psum((first_sum, second_sum), "tp")
    channels_all = channels * tp_size
    center = first_sum / channels_all
    variance = jnp.maximum(second_sum / channels_all - center * center, 0.0)
    normed = (filtered - center[:, None]) * lax.rsqrt(variance + TINY_VAR)[
        :, None
    ] * ln_gain + ln_shift
    conv_mixed = (jax.nn.silu(normed) * jax.nn.silu(conv_gate_raw.astype(jnp.float32))).astype(
        jnp.bfloat16
    )
    summed = jnp.dot(delta_mixed, out_delta, preferred_element_type=jnp.float32)
    return lax.psum_scatter(
        (summed + jnp.dot(conv_mixed, out_conv, preferred_element_type=jnp.float32)).astype(
            jnp.bfloat16
        ),
        "tp",
        scatter_dimension=0,
        tiled=True,
    )


def solution(mesh):
    return jax.shard_map(
        local,
        mesh=mesh,
        in_specs=(
            P("sp", "tp"),
            P(None, "tp"),
            P(None, "tp"),
            P(None, "tp"),
            P(None, "tp"),
            P(None, "tp"),
            P(None, "tp"),
            P(None, "tp"),
            P(),
            P(),
            P(),
            P(),
            P(None, "tp"),
            P("tp"),
            P("tp"),
            P("tp", None),
            P("tp", None),
        ),
        out_specs=P(("sp", "tp"), None),
        check_vma=False,
    )
```

```python
import functools

import jax
import jax.numpy as jnp
from jax import lax
from jax.experimental import pallas as pl
from jax.experimental.pallas import tpu as pltpu
from jax.sharding import PartitionSpec as P

BLOCK = 128
CHUNKS = 4
CUTS = 4


TINY_NORM = 1e-06
TINY_VAR = 1e-05
HIGHEST = lax.Precision.HIGHEST


def shifted(block, axis, distance):
    devices = range(lax.axis_size(axis))
    route = [(i - distance, i) for i in devices if i - distance in devices]
    return lax.ppermute(block, axis, route)


def nt(a, b):
    return lax.dot_general(a, b, (((1,), (1,)), ((), ())), preferred_element_type=jnp.float32)


def mm(a, b):
    return jnp.dot(
        a.astype(jnp.bfloat16), b.astype(jnp.bfloat16), preferred_element_type=jnp.float32
    )


def delta_kernel(
    heads, width, q_ref, k_ref, v_ref, g_ref, outa_ref, outb_ref, final_ref,
    lhs_s, corr_s, score_s, wt_s, tail_s, state_ref,
):
    rows = q_ref.shape[0]
    blocks = rows // BLOCK
    row_id = lax.broadcasted_iota(jnp.int32, (BLOCK, BLOCK), 0)
    col_id = lax.broadcasted_iota(jnp.int32, (BLOCK, BLOCK), 1)
    causal = row_id >= col_id
    strict = row_id > col_id
    differ = row_id ^ col_id
    eye = jnp.where(row_id == col_id, 1.0, 0.0)
    tril = jnp.where(causal, 1.0, 0.0)

    def prepare(c):
        at = pl.ds(pl.multiple_of(c * BLOCK, BLOCK), BLOCK)
        gates = g_ref[at, :]
        sums = jnp.dot(tril, gates, precision=HIGHEST, preferred_element_type=jnp.float32)
        chains = []
        for h in range(heads):
            lanes = slice(h * width, (h + 1) * width)
            k, q = k_ref[at, lanes], q_ref[at, lanes]
            v = v_ref[at, lanes].astype(jnp.float32)
            kf, qf = k.astype(jnp.float32), q.astype(jnp.float32)
            ik = lax.rsqrt(jnp.sum(kf * kf, axis=-1, keepdims=True) + TINY_NORM)
            iq = lax.rsqrt(jnp.sum(qf * qf, axis=-1, keepdims=True) + TINY_NORM)
            iq = iq * width ** (-0.5)
            beta = gates[:, h : h + 1]
            log_sum = sums[:, heads + h : heads + h + 1]
            log_full = jnp.broadcast_to(log_sum, (BLOCK, BLOCK))
            spread = log_full - log_full.T
            damp = jnp.where(causal, jnp.exp(jnp.where(causal, spread, 0.0)), 0.0)
            damp = damp * jnp.broadcast_to(ik, (BLOCK, BLOCK)).T
            lower = jnp.where(strict, nt(k, k) * damp * (beta * ik), 0.0)
            score_s[h, at, :] = (nt(q, k) * damp * iq).astype(jnp.bfloat16)
            grow = jnp.exp(log_sum)
            right = jnp.concatenate([v * beta, kf * (beta * ik * grow)], axis=1)
            tail = log_full[BLOCK - 1 : BLOCK, :]
            weighted = kf * (ik * jnp.exp(tail[:, :1] - log_sum))
            wt_s[h, c] = weighted.T.astype(jnp.bfloat16)
            tail_s[h, c] = jnp.broadcast_to(jnp.exp(tail), (8, BLOCK))
            lhs_s[h, c, BLOCK:, :] = (qf * (iq * grow)).astype(jnp.bfloat16)
            chains.append([h, lower, right, eye - jnp.where(differ == 1, lower, 0.0)])
        return at, c, chains

    def pair(p, carry):
        prepared = [prepare(p * 2 + i) for i in range(2)]
        size = 2
        while size < BLOCK:
            level = (differ >= size) & (differ < 2 * size)
            parts = [
                [mm(jnp.where(level, ch[1], 0.0), ch[3]) for ch in item[2]] for item in prepared
            ]
            for item, part in zip(prepared, parts):
                for ch, moved in zip(item[2], part):
                    ch[3] = ch[3] - mm(ch[3], moved)
            size *= 2
        for at, c, chains in prepared:
            for h, lower, right, inverse in chains:
                solved = mm(inverse, right)
                corr_s[h, at, :] = solved[:, :width]
                lhs_s[h, c, :BLOCK, :] = solved[:, width:].astype(jnp.bfloat16)
        return carry

    lax.fori_loop(0, blocks // 2, pair, 0)
    for h in range(heads):
        state_ref[h] = jnp.concatenate([eye, jnp.zeros((width, width), jnp.float32)], axis=1)

    def advance(c, carry):
        at = pl.ds(pl.multiple_of(c * BLOCK, BLOCK), BLOCK)
        boths = [mm(lhs_s[h, c], state_ref[h]) for h in range(heads)]
        fresh = []
        for h in range(heads):
            first = boths[h][:BLOCK]
            fresh.append(
                jnp.concatenate(
                    [-first[:, :width], corr_s[h, at, :] - first[:, width:]], axis=1
                ).astype(jnp.bfloat16)
            )
        for h in range(heads):
            decay = tail_s[h, c][:1, :]
            decay = jnp.concatenate([decay, decay], axis=1)
            state_ref[h] = state_ref[h] * decay + mm(wt_s[h, c], fresh[h])
        for h in range(heads):
            out = boths[h][BLOCK:] + mm(score_s[h, at, :], fresh[h])
            outa_ref[h, at, :] = out[:, :width].astype(jnp.bfloat16)
            outb_ref[h, at, :] = out[:, width:]
        return carry

    lax.fori_loop(0, blocks, advance, 0)
    final_ref[...] = state_ref[...].astype(jnp.bfloat16)


def delta_rule(query_raw, key_raw, value_raw, gates, heads, width):
    rows = query_raw.shape[0]
    blocks = rows // BLOCK
    vm = pl.BlockSpec(memory_space=pltpu.VMEM)
    return pl.pallas_call(
        functools.partial(delta_kernel, heads, width),
        out_shape=(
            jax.ShapeDtypeStruct((heads, rows, width), jnp.bfloat16),
            jax.ShapeDtypeStruct((heads, rows, width), jnp.float32),
            jax.ShapeDtypeStruct((heads, width, 2 * width), jnp.bfloat16),
        ),
        in_specs=[vm] * 4,
        out_specs=(vm, vm, vm),
        scratch_shapes=[
            pltpu.VMEM((heads, blocks, 2 * BLOCK, width), jnp.bfloat16),
            pltpu.VMEM((heads, rows, width), jnp.float32),
            pltpu.VMEM((heads, rows, BLOCK), jnp.bfloat16),
            pltpu.VMEM((heads, blocks, width, BLOCK), jnp.bfloat16),
            pltpu.VMEM((heads, blocks, 8, BLOCK), jnp.float32),
            pltpu.VMEM((heads, width, 2 * width), jnp.float32),
        ],
        compiler_params=pltpu.CompilerParams(
            vmem_limit_bytes=40 * 1024 * 1024
        ),
        cost_estimate=pl.CostEstimate(
            flops=10_000_000_000, bytes_accessed=4_000_000, transcendentals=0
        ),
        name="delta_rule",
    )(query_raw, key_raw, value_raw, gates)


def finish_kernel(
    heads, width, place_ref, all_ref, outa_ref, outb_ref, gate_ref, gain_ref, mixed_ref, carry_s
):
    rows = outb_ref.shape[1]
    carry_s[...] = jnp.zeros_like(carry_s)

    def hop(i, carry):
        moved = [
            mm(all_ref[i, h, :, :width], carry_s[h])
            for h in range(heads)
        ]
        for h in range(heads):
            carry_s[h] = moved[h] + all_ref[i, h, :, width:].astype(jnp.float32)
        return carry

    lax.fori_loop(0, place_ref[0], hop, 0)
    tile = 256

    def one(c, carry):
        at = pl.ds(pl.multiple_of(c * tile, tile), tile)
        for h in range(heads):
            lanes = slice(h * width, (h + 1) * width)
            result = outb_ref[h, at, :] + mm(outa_ref[h, at, :], carry_s[h])
            result = result * lax.rsqrt(
                jnp.mean(result * result, axis=-1, keepdims=True) + TINY_NORM
            )
            gate = gate_ref[at, lanes].astype(jnp.float32)
            mixed_ref[at, lanes] = (result * gain_ref[...] * jax.nn.silu(gate)).astype(
                jnp.bfloat16
            )
        return carry

    lax.fori_loop(0, rows // tile, one, 0)


def finish(place, states, outa, outb, gate, gain, heads, width):
    rows = outb.shape[1]
    vm = pl.BlockSpec(memory_space=pltpu.VMEM)
    return pl.pallas_call(
        functools.partial(finish_kernel, heads, width),
        out_shape=jax.ShapeDtypeStruct((rows, heads * width), jnp.bfloat16),
        in_specs=[pl.BlockSpec(memory_space=pltpu.SMEM)] + [vm] * 5,
        out_specs=vm,
        scratch_shapes=[pltpu.VMEM((heads, width, width), jnp.float32)],
        compiler_params=pltpu.CompilerParams(vmem_limit_bytes=40 * 1024 * 1024),
        cost_estimate=pl.CostEstimate(
            flops=2_000_000_000, bytes_accessed=6_000_000, transcendentals=0
        ),
        name="delta_finish",
    )(place, states, outa, outb, gate, gain)


MESH = pl.DeviceIdType.MESH


def sharded_place():
    tp = lax.axis_size("tp")
    me = lax.axis_index("tp")
    core = lax.rem(me, 2)
    return tp // 2, me, core, me // 2, me + 1 - 2 * core


def greet(chips, core, chip, sibling):
    barrier = pltpu.get_barrier_semaphore()
    pl.semaphore_signal(barrier, inc=1, device_id={"tp": sibling}, device_id_type=MESH)
    for o in range(1, chips):
        there = lax.rem(chip + o, chips) * 2 + core
        pl.semaphore_signal(barrier, inc=1, device_id={"tp": there}, device_id_type=MESH)
    pl.semaphore_wait(barrier, chips)


def project_kernel(heads, *refs):
    count = 7
    tok_ref, w_refs, wg_ref, rate_ref = refs[0], refs[1 : 1 + count], refs[8], refs[9]
    out_refs, gates_ref = refs[10 : 10 + count], refs[17]
    full, y_send, y_recv, own_send, own_recv, fwd_send, fwd_recv = refs[18:]
    rows, part = tok_ref.shape
    step = rows // CHUNKS
    chips, me, core, chip, sibling = sharded_place()

    def columns(owner):
        return pl.ds(pl.multiple_of(owner * part, part), part)

    def at(r):
        return pl.ds(pl.multiple_of(r * step, step), step)

    def across(o, r):
        there = lax.rem(chip + o, chips) * 2 + core
        return pltpu.make_async_remote_copy(
            src_ref=tok_ref.at[at(r), :],
            dst_ref=full.at[at(r), columns(me)],
            send_sem=y_send.at[o - 1, r],
            recv_sem=y_recv.at[o - 1, r],
            device_id={"tp": there},
            device_id_type=MESH,
        )

    def beside(r):
        return pltpu.make_async_remote_copy(
            src_ref=tok_ref.at[at(r), :],
            dst_ref=full.at[at(r), columns(me)],
            send_sem=own_send.at[r],
            recv_sem=own_recv.at[r],
            device_id={"tp": sibling},
            device_id_type=MESH,
        )

    def forward(o, r):
        owner = lax.rem(chip - o + chips, chips) * 2 + core
        block = full.at[at(r), columns(owner)]
        return pltpu.make_async_remote_copy(
            src_ref=block,
            dst_ref=block,
            send_sem=fwd_send.at[o - 1, r],
            recv_sem=fwd_recv.at[o - 1, r],
            device_id={"tp": sibling},
            device_id_type=MESH,
        )

    greet(chips, core, chip, sibling)
    for r in range(CHUNKS):
        for o in range(1, chips):
            across(o, r).start()
    for r in range(CHUNKS):
        beside(r).start()
    full[:, columns(me)] = tok_ref[...]

    def chunk(r, carry):
        for o in range(1, chips):
            across(o, r).wait_recv()
            forward(o, r).start()
        beside(r).wait_recv()
        for o in range(1, chips):
            forward(o, r).wait_recv()
        squares = jnp.zeros((step, 1), jnp.float32)
        for b in range(2 * chips):
            piece = full[at(r), b * part : (b + 1) * part].astype(jnp.float32)
            squares = squares + jnp.sum(piece * piece, axis=1, keepdims=True)
        inv_rms = lax.rsqrt(squares / (part * 2 * chips) + TINY_NORM)
        for w_ref, out_ref in zip(w_refs, out_refs):
            summed = jnp.dot(full[at(r), :], w_ref[...], preferred_element_type=jnp.float32)
            out_ref[at(r), :] = (summed * inv_rms).astype(jnp.bfloat16)
        raw = jnp.dot(full[at(r), :], wg_ref[...], preferred_element_type=jnp.float32) * inv_rms
        lane = lax.broadcasted_iota(jnp.int32, raw.shape, 1)
        softplus = jnp.maximum(raw, 0.0) + jnp.log1p(jnp.exp(-jnp.abs(raw)))
        gates_ref[at(r), :] = jnp.where(lane < heads, jax.nn.sigmoid(raw), -rate_ref[...] * softplus)
        return carry

    lax.fori_loop(0, CHUNKS, chunk, 0)
    for r in range(CHUNKS):
        for o in range(1, chips):
            across(o, r).wait_send()
            forward(o, r).wait_send()
        beside(r).wait_send()


def project(tokens, weights, w_gates, rates, heads):
    rows, part = tokens.shape
    tp = lax.axis_size("tp")
    others = max(tp // 2 - 1, 1)
    vm = pl.BlockSpec(memory_space=pltpu.VMEM)
    dma = pltpu.SemaphoreType.DMA
    return pl.pallas_call(
        functools.partial(project_kernel, heads),
        out_shape=tuple(
            jax.ShapeDtypeStruct((rows, w.shape[1]), jnp.bfloat16) for w in weights
        )
        + (jax.ShapeDtypeStruct((rows, w_gates.shape[1]), jnp.float32),),
        in_specs=[vm] * (3 + len(weights)),
        out_specs=(vm,) * (1 + len(weights)),
        scratch_shapes=[
            pltpu.VMEM((rows, part * tp), jnp.bfloat16),
            dma((others, CHUNKS)),
            dma((others, CHUNKS)),
            dma((CHUNKS,)),
            dma((CHUNKS,)),
            dma((others, CHUNKS)),
            dma((others, CHUNKS)),
        ],
        compiler_params=pltpu.CompilerParams(
            collective_id=0, has_side_effects=True, vmem_limit_bytes=48 * 1024 * 1024
        ),
        cost_estimate=pl.CostEstimate(
            flops=10_000_000_000, bytes_accessed=20_000_000, transcendentals=0
        ),
        name="gather_project",
    )(tokens, *weights, w_gates, rates)


def output_kernel(
    dm_ref, cm_ref, wd_ref, wc_ref, out_ref,
    beside_out, beside_in, across_out, across_in, b_send, b_recv, y_send, y_recv,
):
    chips, me, core, chip, sibling = sharded_place()
    rows = out_ref.shape[0]
    width = out_ref.shape[1] // CUTS

    def cols(n):
        return pl.ds(pl.multiple_of(n * width, width), width)

    def partial(target, n):
        at = pl.ds(pl.multiple_of(target * rows, rows), rows)
        summed = jnp.dot(dm_ref[at, :], wd_ref[:, cols(n)], preferred_element_type=jnp.float32)
        return summed + jnp.dot(
            cm_ref[at, :], wc_ref[:, cols(n)], preferred_element_type=jnp.float32
        )

    def beside(o, n):
        return pltpu.make_async_remote_copy(
            src_ref=beside_out.at[o, n],
            dst_ref=beside_in.at[o, n],
            send_sem=b_send.at[o, n],
            recv_sem=b_recv.at[o, n],
            device_id={"tp": sibling},
            device_id_type=MESH,
        )

    def across(o, n):
        there = lax.rem(chip + o, chips) * 2 + core
        return pltpu.make_async_remote_copy(
            src_ref=across_out.at[o - 1, n],
            dst_ref=across_in.at[o - 1, n],
            send_sem=y_send.at[o - 1, n],
            recv_sem=y_recv.at[o - 1, n],
            device_id={"tp": there},
            device_id_type=MESH,
        )

    greet(chips, core, chip, sibling)
    order = list(range(1, chips)) + [0]
    for o in order:
        their_chip = lax.rem(chip + o, chips) * 2

        def give(n, carry, o=o, their_chip=their_chip):
            beside_out[o, n] = partial(their_chip + 1 - core, n).astype(jnp.bfloat16)
            beside(o, n).start()
            return carry

        def keep(n, carry, o=o, their_chip=their_chip):
            mine = partial(their_chip + core, n)
            beside(o, n).wait_recv()
            mine = mine + beside_in[o, n].astype(jnp.float32)
            across_out[o - 1, n] = mine.astype(jnp.bfloat16)
            across(o, n).start()
            return carry

        if o != 0:

            def both(n, carry, give=give, keep=keep):
                @pl.when(n + 1 < CUTS)
                def _():
                    give(n + 1, 0)

                return keep(n, carry)

            give(0, 0)
            lax.fori_loop(0, CUTS, both, 0)
        else:
            lax.fori_loop(0, CUTS, give, 0)

    def close(n, carry):
        mine = partial(me, n)
        beside(0, n).wait_recv()
        mine = mine + beside_in[0, n].astype(jnp.float32)
        for o in range(1, chips):
            across(o, n).wait_recv()
            mine = mine + across_in[o - 1, n].astype(jnp.float32)
        out_ref[:, cols(n)] = mine.astype(jnp.bfloat16)
        return carry

    lax.fori_loop(0, CUTS, close, 0)

    def drain(n, carry):
        for o in range(chips):
            beside(o, n).wait_send()
        for o in range(1, chips):
            across(o, n).wait_send()
        return carry

    lax.fori_loop(0, CUTS, drain, 0)


def output_projection(delta_mixed, conv_mixed, out_delta, out_conv):
    tp = lax.axis_size("tp")
    chips = tp // 2
    others = max(chips - 1, 1)
    rows = delta_mixed.shape[0] // tp
    width = out_delta.shape[1]
    cut = width // CUTS
    vm = pl.BlockSpec(memory_space=pltpu.VMEM)
    dma = pltpu.SemaphoreType.DMA
    return pl.pallas_call(
        output_kernel,
        out_shape=jax.ShapeDtypeStruct((rows, width), jnp.bfloat16),
        in_specs=[vm] * 4,
        out_specs=vm,
        scratch_shapes=[
            pltpu.VMEM((chips, CUTS, rows, cut), jnp.bfloat16),
            pltpu.VMEM((chips, CUTS, rows, cut), jnp.bfloat16),
            pltpu.VMEM((others, CUTS, rows, cut), jnp.bfloat16),
            pltpu.VMEM((others, CUTS, rows, cut), jnp.bfloat16),
            dma((chips, CUTS)),
            dma((chips, CUTS)),
            dma((others, CUTS)),
            dma((others, CUTS)),
        ],
        compiler_params=pltpu.CompilerParams(
            collective_id=1, has_side_effects=True, vmem_limit_bytes=48 * 1024 * 1024
        ),
        cost_estimate=pl.CostEstimate(
            flops=10_000_000_000, bytes_accessed=20_000_000, transcendentals=0
        ),
        name="output_scatter",
    )(delta_mixed, conv_mixed, out_delta, out_conv)


def local(
    tokens,
    w_query,
    w_key,
    w_value,
    w_delta_gate,
    w_glu_value,
    w_glu_gate,
    w_conv_gate,
    w_beta,
    w_decay,
    decay_log,
    head_gain,
    conv_taps,
    ln_gain,
    ln_shift,
    out_delta,
    out_conv,
):
    rows_here = tokens.shape[0]
    tp_size = lax.axis_size("tp")
    head_size = head_gain.shape[0]
    heads_here = w_query.shape[1] // head_size
    first_head = lax.axis_index("tp") * heads_here
    rates = jnp.exp(lax.dynamic_slice_in_dim(decay_log, first_head, heads_here, 0))
    fill = head_size - 2 * heads_here
    rates = jnp.concatenate(
        [jnp.zeros((heads_here,), jnp.float32), rates, jnp.zeros((fill,), jnp.float32)]
    )[None, :]
    w_gates = jnp.concatenate(
        [
            lax.dynamic_slice_in_dim(w_beta, first_head, heads_here, 1),
            lax.dynamic_slice_in_dim(w_decay, first_head, heads_here, 1),
            jnp.zeros((w_beta.shape[0], fill), jnp.bfloat16),
        ],
        axis=1,
    )
    weights = (w_query, w_key, w_value, w_delta_gate, w_glu_value, w_glu_gate, w_conv_gate)
    (
        query_raw,
        key_raw,
        value_raw,
        delta_gate_raw,
        glu_value_raw,
        glu_gate_raw,
        conv_gate_raw,
        gates,
    ) = project(tokens, weights, w_gates, rates, heads_here)
    outa, outb, final = delta_rule(
        query_raw, key_raw, value_raw, gates, heads_here, head_size
    )
    states = lax.all_gather(final, "sp")
    place = lax.axis_index("sp").astype(jnp.int32).reshape(1)
    delta_mixed = finish(
        place, states, outa, outb, delta_gate_raw, head_gain[None, :], heads_here, head_size
    )
    kernel = conv_taps.shape[0]
    channels = conv_taps.shape[1]
    gated_units = (
        glu_value_raw.astype(jnp.float32) * jax.nn.sigmoid(glu_gate_raw.astype(jnp.float32))
    ).astype(jnp.bfloat16)
    before = shifted(gated_units[rows_here - (kernel - 1) :], "sp", 1)
    padded = jnp.concatenate([before, gated_units], axis=0)
    filtered = jnp.zeros((rows_here, channels), jnp.float32)
    for offset in range(kernel):
        filtered = filtered + padded[offset : offset + rows_here].astype(jnp.float32) * conv_taps[
            offset
        ].astype(jnp.float32)
    first_sum = jnp.sum(filtered, axis=1)
    second_sum = jnp.sum(filtered * filtered, axis=1)
    first_sum, second_sum = lax.psum((first_sum, second_sum), "tp")
    channels_all = channels * tp_size
    center = first_sum / channels_all
    variance = jnp.maximum(second_sum / channels_all - center * center, 0.0)
    normed = (filtered - center[:, None]) * lax.rsqrt(variance + TINY_VAR)[
        :, None
    ] * ln_gain + ln_shift
    conv_mixed = (jax.nn.silu(normed) * jax.nn.silu(conv_gate_raw.astype(jnp.float32))).astype(
        jnp.bfloat16
    )
    return output_projection(delta_mixed, conv_mixed, out_delta, out_conv)


def solution(mesh):
    return jax.shard_map(
        local,
        mesh=mesh,
        in_specs=(
            P("sp", "tp"),
            P(None, "tp"),
            P(None, "tp"),
            P(None, "tp"),
            P(None, "tp"),
            P(None, "tp"),
            P(None, "tp"),
            P(None, "tp"),
            P(),
            P(),
            P(),
            P(),
            P(None, "tp"),
            P("tp"),
            P("tp"),
            P("tp", None),
            P("tp", None),
        ),
        out_specs=P(("sp", "tp"), None),
        check_vma=False,
    )
```

```python
import functools

import jax
import jax.numpy as jnp
from jax import lax
from jax.experimental import pallas as pl
from jax.experimental.pallas import tpu as pltpu
from jax.sharding import PartitionSpec as P

BLOCK = 128
CHUNKS = 4
CUTS = 4


TINY_NORM = 1e-06
TINY_VAR = 1e-05
HIGHEST = lax.Precision.HIGHEST


def shifted(block, axis, distance):
    devices = range(lax.axis_size(axis))
    route = [(i - distance, i) for i in devices if i - distance in devices]
    return lax.ppermute(block, axis, route)


def compose(later, earlier, width):
    moved = jnp.einsum(
        "hij,hjk->hik",
        later[..., :width].astype(jnp.bfloat16),
        earlier,
        preferred_element_type=jnp.float32,
    )
    return moved + jnp.concatenate(
        [jnp.zeros_like(later[..., :width]), later[..., width:]], axis=-1
    ).astype(jnp.float32)


def entering(final, axis, width):
    devices = lax.axis_size(axis)
    window = compose(shifted(final, axis, 1), shifted(final, axis, 2), width)
    reach = 2
    while 2 * reach < devices:
        earlier = shifted(window.astype(jnp.bfloat16), axis, reach)
        window = compose(window, earlier, width)
        reach *= 2
    return window, shifted(window[..., width:].astype(jnp.bfloat16), axis, reach)


def nt(a, b):
    return lax.dot_general(a, b, (((1,), (1,)), ((), ())), preferred_element_type=jnp.float32)


def mm(a, b):
    return jnp.dot(
        a.astype(jnp.bfloat16), b.astype(jnp.bfloat16), preferred_element_type=jnp.float32
    )


def delta_kernel(
    heads, width, q_ref, k_ref, v_ref, g_ref, outa_ref, outb_ref, final_ref,
    lhs_s, corr_s, score_s, wt_s, tail_s, state_ref,
):
    rows = q_ref.shape[0]
    blocks = rows // BLOCK
    row_id = lax.broadcasted_iota(jnp.int32, (BLOCK, BLOCK), 0)
    col_id = lax.broadcasted_iota(jnp.int32, (BLOCK, BLOCK), 1)
    causal = row_id >= col_id
    strict = row_id > col_id
    differ = row_id ^ col_id
    eye = jnp.where(row_id == col_id, 1.0, 0.0)
    tril = jnp.where(causal, 1.0, 0.0)

    def prepare(c):
        at = pl.ds(pl.multiple_of(c * BLOCK, BLOCK), BLOCK)
        gates = g_ref[at, :]
        sums = jnp.dot(tril, gates, precision=HIGHEST, preferred_element_type=jnp.float32)
        chains = []
        for h in range(heads):
            lanes = slice(h * width, (h + 1) * width)
            k, q = k_ref[at, lanes], q_ref[at, lanes]
            v = v_ref[at, lanes].astype(jnp.float32)
            kf, qf = k.astype(jnp.float32), q.astype(jnp.float32)
            ik = lax.rsqrt(jnp.sum(kf * kf, axis=-1, keepdims=True) + TINY_NORM)
            iq = lax.rsqrt(jnp.sum(qf * qf, axis=-1, keepdims=True) + TINY_NORM)
            iq = iq * width ** (-0.5)
            beta = gates[:, h : h + 1]
            log_sum = sums[:, heads + h : heads + h + 1]
            log_full = jnp.broadcast_to(log_sum, (BLOCK, BLOCK))
            spread = log_full - log_full.T
            damp = jnp.where(causal, jnp.exp(jnp.where(causal, spread, 0.0)), 0.0)
            damp = damp * jnp.broadcast_to(ik, (BLOCK, BLOCK)).T
            lower = jnp.where(strict, nt(k, k) * damp * (beta * ik), 0.0)
            score_s[h, at, :] = (nt(q, k) * damp * iq).astype(jnp.bfloat16)
            grow = jnp.exp(log_sum)
            right = jnp.concatenate([v * beta, kf * (beta * ik * grow)], axis=1)
            tail = log_full[BLOCK - 1 : BLOCK, :]
            weighted = kf * (ik * jnp.exp(tail[:, :1] - log_sum))
            wt_s[h, c] = weighted.T.astype(jnp.bfloat16)
            tail_s[h, c] = jnp.broadcast_to(jnp.exp(tail), (8, BLOCK))
            lhs_s[h, c, BLOCK:, :] = (qf * (iq * grow)).astype(jnp.bfloat16)
            chains.append([h, lower, right, eye - jnp.where(differ == 1, lower, 0.0)])
        return at, c, chains

    def pair(p, carry):
        prepared = [prepare(p * 2 + i) for i in range(2)]
        size = 2
        while size < BLOCK:
            level = (differ >= size) & (differ < 2 * size)
            parts = [
                [mm(jnp.where(level, ch[1], 0.0), ch[3]) for ch in item[2]] for item in prepared
            ]
            for item, part in zip(prepared, parts):
                for ch, moved in zip(item[2], part):
                    ch[3] = ch[3] - mm(ch[3], moved)
            size *= 2
        for at, c, chains in prepared:
            for h, lower, right, inverse in chains:
                solved = mm(inverse, right)
                corr_s[h, at, :] = solved[:, :width]
                lhs_s[h, c, :BLOCK, :] = solved[:, width:].astype(jnp.bfloat16)
        return carry

    lax.fori_loop(0, blocks // 2, pair, 0)
    for h in range(heads):
        state_ref[h] = jnp.concatenate([eye, jnp.zeros((width, width), jnp.float32)], axis=1)

    def advance(c, carry):
        at = pl.ds(pl.multiple_of(c * BLOCK, BLOCK), BLOCK)
        boths = [mm(lhs_s[h, c], state_ref[h]) for h in range(heads)]
        fresh = []
        for h in range(heads):
            first = boths[h][:BLOCK]
            fresh.append(
                jnp.concatenate(
                    [-first[:, :width], corr_s[h, at, :] - first[:, width:]], axis=1
                ).astype(jnp.bfloat16)
            )
        for h in range(heads):
            decay = tail_s[h, c][:1, :]
            decay = jnp.concatenate([decay, decay], axis=1)
            state_ref[h] = state_ref[h] * decay + mm(wt_s[h, c], fresh[h])
        for h in range(heads):
            out = boths[h][BLOCK:] + mm(score_s[h, at, :], fresh[h])
            outa_ref[h, at, :] = out[:, :width].astype(jnp.bfloat16)
            outb_ref[h, at, :] = out[:, width:]
        return carry

    lax.fori_loop(0, blocks, advance, 0)
    final_ref[...] = state_ref[...].astype(jnp.bfloat16)


def delta_rule(query_raw, key_raw, value_raw, gates, heads, width):
    rows = query_raw.shape[0]
    blocks = rows // BLOCK
    vm = pl.BlockSpec(memory_space=pltpu.VMEM)
    return pl.pallas_call(
        functools.partial(delta_kernel, heads, width),
        out_shape=(
            jax.ShapeDtypeStruct((heads, rows, width), jnp.bfloat16),
            jax.ShapeDtypeStruct((heads, rows, width), jnp.float32),
            jax.ShapeDtypeStruct((heads, width, 2 * width), jnp.bfloat16),
        ),
        in_specs=[vm] * 4,
        out_specs=(vm, vm, vm),
        scratch_shapes=[
            pltpu.VMEM((heads, blocks, 2 * BLOCK, width), jnp.bfloat16),
            pltpu.VMEM((heads, rows, width), jnp.float32),
            pltpu.VMEM((heads, rows, BLOCK), jnp.bfloat16),
            pltpu.VMEM((heads, blocks, width, BLOCK), jnp.bfloat16),
            pltpu.VMEM((heads, blocks, 8, BLOCK), jnp.float32),
            pltpu.VMEM((heads, width, 2 * width), jnp.float32),
        ],
        compiler_params=pltpu.CompilerParams(
            vmem_limit_bytes=40 * 1024 * 1024
        ),
        cost_estimate=pl.CostEstimate(
            flops=10_000_000_000, bytes_accessed=4_000_000, transcendentals=0
        ),
        name="delta_rule",
    )(query_raw, key_raw, value_raw, gates)


def finish_kernel(
    heads, width, window_ref, earlier_ref, outa_ref, outb_ref, gate_ref, gain_ref, mixed_ref
):
    rows = outb_ref.shape[1]
    carried = [
        mm(window_ref[h, :, :width], earlier_ref[h]) + window_ref[h, :, width:]
        for h in range(heads)
    ]
    carried = [item.astype(jnp.bfloat16) for item in carried]
    tile = 256

    def one(c, carry):
        at = pl.ds(pl.multiple_of(c * tile, tile), tile)
        for h in range(heads):
            lanes = slice(h * width, (h + 1) * width)
            result = outb_ref[h, at, :] + mm(outa_ref[h, at, :], carried[h])
            result = result * lax.rsqrt(
                jnp.mean(result * result, axis=-1, keepdims=True) + TINY_NORM
            )
            gate = gate_ref[at, lanes].astype(jnp.float32)
            mixed_ref[at, lanes] = (result * gain_ref[...] * jax.nn.silu(gate)).astype(
                jnp.bfloat16
            )
        return carry

    lax.fori_loop(0, rows // tile, one, 0)


def finish(window, earlier, outa, outb, gate, gain, heads, width):
    rows = outb.shape[1]
    vm = pl.BlockSpec(memory_space=pltpu.VMEM)
    return pl.pallas_call(
        functools.partial(finish_kernel, heads, width),
        out_shape=jax.ShapeDtypeStruct((rows, heads * width), jnp.bfloat16),
        in_specs=[vm] * 6,
        out_specs=vm,
        compiler_params=pltpu.CompilerParams(vmem_limit_bytes=40 * 1024 * 1024),
        cost_estimate=pl.CostEstimate(
            flops=2_000_000_000, bytes_accessed=6_000_000, transcendentals=0
        ),
        name="delta_finish",
    )(window, earlier, outa, outb, gate, gain)


MESH = pl.DeviceIdType.MESH


def sharded_place():
    tp = lax.axis_size("tp")
    me = lax.axis_index("tp")
    core = lax.rem(me, 2)
    return tp // 2, me, core, me // 2, me + 1 - 2 * core


def greet(chips, core, chip, sibling):
    barrier = pltpu.get_barrier_semaphore()
    pl.semaphore_signal(barrier, inc=1, device_id={"tp": sibling}, device_id_type=MESH)
    for o in range(1, chips):
        there = lax.rem(chip + o, chips) * 2 + core
        pl.semaphore_signal(barrier, inc=1, device_id={"tp": there}, device_id_type=MESH)
    pl.semaphore_wait(barrier, chips)


def project_kernel(heads, *refs):
    count = 7
    tok_ref, w_refs, wg_ref, rate_ref = refs[0], refs[1 : 1 + count], refs[8], refs[9]
    out_refs, gates_ref = refs[10 : 10 + count], refs[17]
    full, y_send, y_recv, own_send, own_recv, fwd_send, fwd_recv = refs[18:]
    rows, part = tok_ref.shape
    step = rows // CHUNKS
    chips, me, core, chip, sibling = sharded_place()

    def columns(owner):
        return pl.ds(pl.multiple_of(owner * part, part), part)

    def at(r):
        return pl.ds(pl.multiple_of(r * step, step), step)

    def across(o, r):
        there = lax.rem(chip + o, chips) * 2 + core
        return pltpu.make_async_remote_copy(
            src_ref=tok_ref.at[at(r), :],
            dst_ref=full.at[at(r), columns(me)],
            send_sem=y_send.at[o - 1, r],
            recv_sem=y_recv.at[o - 1, r],
            device_id={"tp": there},
            device_id_type=MESH,
        )

    def beside(r):
        return pltpu.make_async_remote_copy(
            src_ref=tok_ref.at[at(r), :],
            dst_ref=full.at[at(r), columns(me)],
            send_sem=own_send.at[r],
            recv_sem=own_recv.at[r],
            device_id={"tp": sibling},
            device_id_type=MESH,
        )

    def forward(o, r):
        owner = lax.rem(chip - o + chips, chips) * 2 + core
        block = full.at[at(r), columns(owner)]
        return pltpu.make_async_remote_copy(
            src_ref=block,
            dst_ref=block,
            send_sem=fwd_send.at[o - 1, r],
            recv_sem=fwd_recv.at[o - 1, r],
            device_id={"tp": sibling},
            device_id_type=MESH,
        )

    greet(chips, core, chip, sibling)
    for r in range(CHUNKS):
        for o in range(1, chips):
            across(o, r).start()
    for r in range(CHUNKS):
        beside(r).start()
    full[:, columns(me)] = tok_ref[...]

    def chunk(r, carry):
        for o in range(1, chips):
            across(o, r).wait_recv()
            forward(o, r).start()
        beside(r).wait_recv()
        for o in range(1, chips):
            forward(o, r).wait_recv()
        squares = jnp.zeros((step, 1), jnp.float32)
        for b in range(2 * chips):
            piece = full[at(r), b * part : (b + 1) * part].astype(jnp.float32)
            squares = squares + jnp.sum(piece * piece, axis=1, keepdims=True)
        inv_rms = lax.rsqrt(squares / (part * 2 * chips) + TINY_NORM)
        for w_ref, out_ref in zip(w_refs, out_refs):
            summed = jnp.dot(full[at(r), :], w_ref[...], preferred_element_type=jnp.float32)
            out_ref[at(r), :] = (summed * inv_rms).astype(jnp.bfloat16)
        raw = jnp.dot(full[at(r), :], wg_ref[...], preferred_element_type=jnp.float32) * inv_rms
        lane = lax.broadcasted_iota(jnp.int32, raw.shape, 1)
        softplus = jnp.maximum(raw, 0.0) + jnp.log1p(jnp.exp(-jnp.abs(raw)))
        gates_ref[at(r), :] = jnp.where(lane < heads, jax.nn.sigmoid(raw), -rate_ref[...] * softplus)
        return carry

    lax.fori_loop(0, CHUNKS, chunk, 0)
    for r in range(CHUNKS):
        for o in range(1, chips):
            across(o, r).wait_send()
            forward(o, r).wait_send()
        beside(r).wait_send()


def project(tokens, weights, w_gates, rates, heads):
    rows, part = tokens.shape
    tp = lax.axis_size("tp")
    others = max(tp // 2 - 1, 1)
    vm = pl.BlockSpec(memory_space=pltpu.VMEM)
    dma = pltpu.SemaphoreType.DMA
    return pl.pallas_call(
        functools.partial(project_kernel, heads),
        out_shape=tuple(
            jax.ShapeDtypeStruct((rows, w.shape[1]), jnp.bfloat16) for w in weights
        )
        + (jax.ShapeDtypeStruct((rows, w_gates.shape[1]), jnp.float32),),
        in_specs=[vm] * (3 + len(weights)),
        out_specs=(vm,) * (1 + len(weights)),
        scratch_shapes=[
            pltpu.VMEM((rows, part * tp), jnp.bfloat16),
            dma((others, CHUNKS)),
            dma((others, CHUNKS)),
            dma((CHUNKS,)),
            dma((CHUNKS,)),
            dma((others, CHUNKS)),
            dma((others, CHUNKS)),
        ],
        compiler_params=pltpu.CompilerParams(
            collective_id=0, has_side_effects=True, vmem_limit_bytes=48 * 1024 * 1024
        ),
        cost_estimate=pl.CostEstimate(
            flops=10_000_000_000, bytes_accessed=20_000_000, transcendentals=0
        ),
        name="gather_project",
    )(tokens, *weights, w_gates, rates)


def output_kernel(
    dm_ref, cm_ref, wd_ref, wc_ref, out_ref,
    beside_out, beside_in, across_out, across_in, b_send, b_recv, y_send, y_recv,
):
    chips, me, core, chip, sibling = sharded_place()
    rows = out_ref.shape[0]
    width = out_ref.shape[1] // CUTS

    def cols(n):
        return pl.ds(pl.multiple_of(n * width, width), width)

    def partial(target, n):
        at = pl.ds(pl.multiple_of(target * rows, rows), rows)
        summed = jnp.dot(dm_ref[at, :], wd_ref[:, cols(n)], preferred_element_type=jnp.float32)
        return summed + jnp.dot(
            cm_ref[at, :], wc_ref[:, cols(n)], preferred_element_type=jnp.float32
        )

    def beside(o, n):
        return pltpu.make_async_remote_copy(
            src_ref=beside_out.at[o, n],
            dst_ref=beside_in.at[o, n],
            send_sem=b_send.at[o, n],
            recv_sem=b_recv.at[o, n],
            device_id={"tp": sibling},
            device_id_type=MESH,
        )

    def across(o, n):
        there = lax.rem(chip + o, chips) * 2 + core
        return pltpu.make_async_remote_copy(
            src_ref=across_out.at[o - 1, n],
            dst_ref=across_in.at[o - 1, n],
            send_sem=y_send.at[o - 1, n],
            recv_sem=y_recv.at[o - 1, n],
            device_id={"tp": there},
            device_id_type=MESH,
        )

    greet(chips, core, chip, sibling)
    order = list(range(1, chips)) + [0]
    for o in order:
        their_chip = lax.rem(chip + o, chips) * 2

        def give(n, carry, o=o, their_chip=their_chip):
            beside_out[o, n] = partial(their_chip + 1 - core, n).astype(jnp.bfloat16)
            beside(o, n).start()
            return carry

        def keep(n, carry, o=o, their_chip=their_chip):
            mine = partial(their_chip + core, n)
            beside(o, n).wait_recv()
            mine = mine + beside_in[o, n].astype(jnp.float32)
            across_out[o - 1, n] = mine.astype(jnp.bfloat16)
            across(o, n).start()
            return carry

        if o != 0:

            def both(n, carry, give=give, keep=keep):
                @pl.when(n + 1 < CUTS)
                def _():
                    give(n + 1, 0)

                return keep(n, carry)

            give(0, 0)
            lax.fori_loop(0, CUTS, both, 0)
        else:
            lax.fori_loop(0, CUTS, give, 0)

    def close(n, carry):
        mine = partial(me, n)
        beside(0, n).wait_recv()
        mine = mine + beside_in[0, n].astype(jnp.float32)
        for o in range(1, chips):
            across(o, n).wait_recv()
            mine = mine + across_in[o - 1, n].astype(jnp.float32)
        out_ref[:, cols(n)] = mine.astype(jnp.bfloat16)
        return carry

    lax.fori_loop(0, CUTS, close, 0)

    def drain(n, carry):
        for o in range(chips):
            beside(o, n).wait_send()
        for o in range(1, chips):
            across(o, n).wait_send()
        return carry

    lax.fori_loop(0, CUTS, drain, 0)


def output_projection(delta_mixed, conv_mixed, out_delta, out_conv):
    tp = lax.axis_size("tp")
    chips = tp // 2
    others = max(chips - 1, 1)
    rows = delta_mixed.shape[0] // tp
    width = out_delta.shape[1]
    cut = width // CUTS
    vm = pl.BlockSpec(memory_space=pltpu.VMEM)
    dma = pltpu.SemaphoreType.DMA
    return pl.pallas_call(
        output_kernel,
        out_shape=jax.ShapeDtypeStruct((rows, width), jnp.bfloat16),
        in_specs=[vm] * 4,
        out_specs=vm,
        scratch_shapes=[
            pltpu.VMEM((chips, CUTS, rows, cut), jnp.bfloat16),
            pltpu.VMEM((chips, CUTS, rows, cut), jnp.bfloat16),
            pltpu.VMEM((others, CUTS, rows, cut), jnp.bfloat16),
            pltpu.VMEM((others, CUTS, rows, cut), jnp.bfloat16),
            dma((chips, CUTS)),
            dma((chips, CUTS)),
            dma((others, CUTS)),
            dma((others, CUTS)),
        ],
        compiler_params=pltpu.CompilerParams(
            collective_id=1, has_side_effects=True, vmem_limit_bytes=48 * 1024 * 1024
        ),
        cost_estimate=pl.CostEstimate(
            flops=10_000_000_000, bytes_accessed=20_000_000, transcendentals=0
        ),
        name="output_scatter",
    )(delta_mixed, conv_mixed, out_delta, out_conv)


def local(
    tokens,
    w_query,
    w_key,
    w_value,
    w_delta_gate,
    w_glu_value,
    w_glu_gate,
    w_conv_gate,
    w_beta,
    w_decay,
    decay_log,
    head_gain,
    conv_taps,
    ln_gain,
    ln_shift,
    out_delta,
    out_conv,
):
    rows_here = tokens.shape[0]
    tp_size = lax.axis_size("tp")
    head_size = head_gain.shape[0]
    heads_here = w_query.shape[1] // head_size
    first_head = lax.axis_index("tp") * heads_here
    rates = jnp.exp(lax.dynamic_slice_in_dim(decay_log, first_head, heads_here, 0))
    fill = head_size - 2 * heads_here
    rates = jnp.concatenate(
        [jnp.zeros((heads_here,), jnp.float32), rates, jnp.zeros((fill,), jnp.float32)]
    )[None, :]
    w_gates = jnp.concatenate(
        [
            lax.dynamic_slice_in_dim(w_beta, first_head, heads_here, 1),
            lax.dynamic_slice_in_dim(w_decay, first_head, heads_here, 1),
            jnp.zeros((w_beta.shape[0], fill), jnp.bfloat16),
        ],
        axis=1,
    )
    weights = (w_query, w_key, w_value, w_delta_gate, w_glu_value, w_glu_gate, w_conv_gate)
    (
        query_raw,
        key_raw,
        value_raw,
        delta_gate_raw,
        glu_value_raw,
        glu_gate_raw,
        conv_gate_raw,
        gates,
    ) = project(tokens, weights, w_gates, rates, heads_here)
    outa, outb, final = delta_rule(
        query_raw, key_raw, value_raw, gates, heads_here, head_size
    )
    window, earlier = entering(final, "sp", head_size)
    delta_mixed = finish(
        window, earlier, outa, outb, delta_gate_raw, head_gain[None, :], heads_here, head_size
    )
    kernel = conv_taps.shape[0]
    channels = conv_taps.shape[1]
    gated_units = (
        glu_value_raw.astype(jnp.float32) * jax.nn.sigmoid(glu_gate_raw.astype(jnp.float32))
    ).astype(jnp.bfloat16)
    before = shifted(gated_units[rows_here - (kernel - 1) :], "sp", 1)
    padded = jnp.concatenate([before, gated_units], axis=0)
    filtered = jnp.zeros((rows_here, channels), jnp.float32)
    for offset in range(kernel):
        filtered = filtered + padded[offset : offset + rows_here].astype(jnp.float32) * conv_taps[
            offset
        ].astype(jnp.float32)
    first_sum = jnp.sum(filtered, axis=1)
    second_sum = jnp.sum(filtered * filtered, axis=1)
    first_sum, second_sum = lax.psum((first_sum, second_sum), "tp")
    channels_all = channels * tp_size
    center = first_sum / channels_all
    variance = jnp.maximum(second_sum / channels_all - center * center, 0.0)
    normed = (filtered - center[:, None]) * lax.rsqrt(variance + TINY_VAR)[
        :, None
    ] * ln_gain + ln_shift
    conv_mixed = (jax.nn.silu(normed) * jax.nn.silu(conv_gate_raw.astype(jnp.float32))).astype(
        jnp.bfloat16
    )
    return output_projection(delta_mixed, conv_mixed, out_delta, out_conv)


def solution(mesh):
    return jax.shard_map(
        local,
        mesh=mesh,
        in_specs=(
            P("sp", "tp"),
            P(None, "tp"),
            P(None, "tp"),
            P(None, "tp"),
            P(None, "tp"),
            P(None, "tp"),
            P(None, "tp"),
            P(None, "tp"),
            P(),
            P(),
            P(),
            P(),
            P(None, "tp"),
            P("tp"),
            P("tp"),
            P("tp", None),
            P("tp", None),
        ),
        out_specs=P(("sp", "tp"), None),
        check_vma=False,
    )
```

```python
import functools

import jax
import jax.numpy as jnp
from jax import lax
from jax.experimental import pallas as pl
from jax.experimental.pallas import tpu as pltpu
from jax.sharding import PartitionSpec as P

BLOCK = 128
CHUNKS = 4
CUTS = 4


TINY_NORM = 1e-06
TINY_VAR = 1e-05
HIGHEST = lax.Precision.HIGHEST


def nt(a, b):
    return lax.dot_general(a, b, (((1,), (1,)), ((), ())), preferred_element_type=jnp.float32)


def mm(a, b):
    return jnp.dot(
        a.astype(jnp.bfloat16), b.astype(jnp.bfloat16), preferred_element_type=jnp.float32
    )


def delta_kernel(
    heads, width, q_ref, k_ref, v_ref, g_ref, outa_ref, outb_ref, final_ref,
    lhs_s, corr_s, score_s, wt_s, tail_s, state_ref,
):
    rows = q_ref.shape[0]
    blocks = rows // BLOCK
    row_id = lax.broadcasted_iota(jnp.int32, (BLOCK, BLOCK), 0)
    col_id = lax.broadcasted_iota(jnp.int32, (BLOCK, BLOCK), 1)
    causal = row_id >= col_id
    strict = row_id > col_id
    differ = row_id ^ col_id
    eye = jnp.where(row_id == col_id, 1.0, 0.0)
    tril = jnp.where(causal, 1.0, 0.0)

    def prepare(c):
        at = pl.ds(pl.multiple_of(c * BLOCK, BLOCK), BLOCK)
        gates = g_ref[at, :]
        sums = jnp.dot(tril, gates, precision=HIGHEST, preferred_element_type=jnp.float32)
        chains = []
        for h in range(heads):
            lanes = slice(h * width, (h + 1) * width)
            k, q = k_ref[at, lanes], q_ref[at, lanes]
            v = v_ref[at, lanes].astype(jnp.float32)
            kf, qf = k.astype(jnp.float32), q.astype(jnp.float32)
            ik = lax.rsqrt(jnp.sum(kf * kf, axis=-1, keepdims=True) + TINY_NORM)
            iq = lax.rsqrt(jnp.sum(qf * qf, axis=-1, keepdims=True) + TINY_NORM)
            iq = iq * width ** (-0.5)
            beta = gates[:, h : h + 1]
            log_sum = sums[:, heads + h : heads + h + 1]
            log_full = jnp.broadcast_to(log_sum, (BLOCK, BLOCK))
            spread = log_full - log_full.T
            damp = jnp.where(causal, jnp.exp(jnp.where(causal, spread, 0.0)), 0.0)
            damp = damp * jnp.broadcast_to(ik, (BLOCK, BLOCK)).T
            lower = jnp.where(strict, nt(k, k) * damp * (beta * ik), 0.0)
            score_s[h, at, :] = (nt(q, k) * damp * iq).astype(jnp.bfloat16)
            grow = jnp.exp(log_sum)
            right = jnp.concatenate([v * beta, kf * (beta * ik * grow)], axis=1)
            tail = log_full[BLOCK - 1 : BLOCK, :]
            weighted = kf * (ik * jnp.exp(tail[:, :1] - log_sum))
            wt_s[h, c] = weighted.T.astype(jnp.bfloat16)
            tail_s[h, c] = jnp.broadcast_to(jnp.exp(tail), (8, BLOCK))
            lhs_s[h, c, BLOCK:, :] = (qf * (iq * grow)).astype(jnp.bfloat16)
            chains.append([h, lower, right, eye - jnp.where(differ == 1, lower, 0.0)])
        return at, c, chains

    def pair(p, carry):
        prepared = [prepare(p * 2 + i) for i in range(2)]
        size = 2
        while size < BLOCK:
            level = (differ >= size) & (differ < 2 * size)
            parts = [
                [mm(jnp.where(level, ch[1], 0.0), ch[3]) for ch in item[2]] for item in prepared
            ]
            for item, part in zip(prepared, parts):
                for ch, moved in zip(item[2], part):
                    ch[3] = ch[3] - mm(ch[3], moved)
            size *= 2
        for at, c, chains in prepared:
            for h, lower, right, inverse in chains:
                solved = mm(inverse, right)
                corr_s[h, at, :] = solved[:, :width]
                lhs_s[h, c, :BLOCK, :] = solved[:, width:].astype(jnp.bfloat16)
        return carry

    lax.fori_loop(0, blocks // 2, pair, 0)
    for h in range(heads):
        state_ref[h] = jnp.concatenate([eye, jnp.zeros((width, width), jnp.float32)], axis=1)

    def advance(c, carry):
        at = pl.ds(pl.multiple_of(c * BLOCK, BLOCK), BLOCK)
        boths = [mm(lhs_s[h, c], state_ref[h]) for h in range(heads)]
        fresh = []
        for h in range(heads):
            first = boths[h][:BLOCK]
            fresh.append(
                jnp.concatenate(
                    [-first[:, :width], corr_s[h, at, :] - first[:, width:]], axis=1
                ).astype(jnp.bfloat16)
            )
        for h in range(heads):
            decay = tail_s[h, c][:1, :]
            decay = jnp.concatenate([decay, decay], axis=1)
            state_ref[h] = state_ref[h] * decay + mm(wt_s[h, c], fresh[h])
        for h in range(heads):
            out = boths[h][BLOCK:] + mm(score_s[h, at, :], fresh[h])
            outa_ref[h, at, :] = out[:, :width].astype(jnp.bfloat16)
            outb_ref[h, at, :] = out[:, width:]
        return carry

    lax.fori_loop(0, blocks, advance, 0)
    final_ref[...] = state_ref[...].astype(jnp.bfloat16)


def delta_rule(query_raw, key_raw, value_raw, gates, heads, width):
    rows = query_raw.shape[0]
    blocks = rows // BLOCK
    vm = pl.BlockSpec(memory_space=pltpu.VMEM)
    return pl.pallas_call(
        functools.partial(delta_kernel, heads, width),
        out_shape=(
            jax.ShapeDtypeStruct((heads, rows, width), jnp.bfloat16),
            jax.ShapeDtypeStruct((heads, rows, width), jnp.float32),
            jax.ShapeDtypeStruct((heads, width, 2 * width), jnp.bfloat16),
        ),
        in_specs=[vm] * 4,
        out_specs=(vm, vm, vm),
        scratch_shapes=[
            pltpu.VMEM((heads, blocks, 2 * BLOCK, width), jnp.bfloat16),
            pltpu.VMEM((heads, rows, width), jnp.float32),
            pltpu.VMEM((heads, rows, BLOCK), jnp.bfloat16),
            pltpu.VMEM((heads, blocks, width, BLOCK), jnp.bfloat16),
            pltpu.VMEM((heads, blocks, 8, BLOCK), jnp.float32),
            pltpu.VMEM((heads, width, 2 * width), jnp.float32),
        ],
        compiler_params=pltpu.CompilerParams(
            vmem_limit_bytes=40 * 1024 * 1024
        ),
        cost_estimate=pl.CostEstimate(
            flops=10_000_000_000, bytes_accessed=4_000_000, transcendentals=0
        ),
        name="delta_rule",
    )(query_raw, key_raw, value_raw, gates)


MESH = pl.DeviceIdType.MESH


def sharded_place():
    tp = lax.axis_size("tp")
    me = lax.axis_index("tp")
    core = lax.rem(me, 2)
    return tp // 2, me, core, me // 2, me + 1 - 2 * core


def greet(chips, core, chip, sibling):
    barrier = pltpu.get_barrier_semaphore()
    pl.semaphore_signal(barrier, inc=1, device_id={"tp": sibling}, device_id_type=MESH)
    for o in range(1, chips):
        there = lax.rem(chip + o, chips) * 2 + core
        pl.semaphore_signal(barrier, inc=1, device_id={"tp": there}, device_id_type=MESH)
    pl.semaphore_wait(barrier, chips)


def project_kernel(heads, *refs):
    count = 7
    tok_ref, w_refs, wg_ref, rate_ref = refs[0], refs[1 : 1 + count], refs[8], refs[9]
    out_refs, gates_ref = refs[10 : 10 + count], refs[17]
    full, y_send, y_recv, own_send, own_recv, fwd_send, fwd_recv = refs[18:]
    rows, part = tok_ref.shape
    step = rows // CHUNKS
    chips, me, core, chip, sibling = sharded_place()

    def columns(owner):
        return pl.ds(pl.multiple_of(owner * part, part), part)

    def at(r):
        return pl.ds(pl.multiple_of(r * step, step), step)

    def across(o, r):
        there = lax.rem(chip + o, chips) * 2 + core
        return pltpu.make_async_remote_copy(
            src_ref=tok_ref.at[at(r), :],
            dst_ref=full.at[at(r), columns(me)],
            send_sem=y_send.at[o - 1, r],
            recv_sem=y_recv.at[o - 1, r],
            device_id={"tp": there},
            device_id_type=MESH,
        )

    def beside(r):
        return pltpu.make_async_remote_copy(
            src_ref=tok_ref.at[at(r), :],
            dst_ref=full.at[at(r), columns(me)],
            send_sem=own_send.at[r],
            recv_sem=own_recv.at[r],
            device_id={"tp": sibling},
            device_id_type=MESH,
        )

    def forward(o, r):
        owner = lax.rem(chip - o + chips, chips) * 2 + core
        block = full.at[at(r), columns(owner)]
        return pltpu.make_async_remote_copy(
            src_ref=block,
            dst_ref=block,
            send_sem=fwd_send.at[o - 1, r],
            recv_sem=fwd_recv.at[o - 1, r],
            device_id={"tp": sibling},
            device_id_type=MESH,
        )

    greet(chips, core, chip, sibling)
    for r in range(CHUNKS):
        for o in range(1, chips):
            across(o, r).start()
    for r in range(CHUNKS):
        beside(r).start()
    full[:, columns(me)] = tok_ref[...]

    def chunk(r, carry):
        for o in range(1, chips):
            across(o, r).wait_recv()
            forward(o, r).start()
        beside(r).wait_recv()
        for o in range(1, chips):
            forward(o, r).wait_recv()
        squares = jnp.zeros((step, 1), jnp.float32)
        for b in range(2 * chips):
            piece = full[at(r), b * part : (b + 1) * part].astype(jnp.float32)
            squares = squares + jnp.sum(piece * piece, axis=1, keepdims=True)
        inv_rms = lax.rsqrt(squares / (part * 2 * chips) + TINY_NORM)
        for w_ref, out_ref in zip(w_refs, out_refs):
            summed = jnp.dot(full[at(r), :], w_ref[...], preferred_element_type=jnp.float32)
            out_ref[at(r), :] = (summed * inv_rms).astype(jnp.bfloat16)
        raw = jnp.dot(full[at(r), :], wg_ref[...], preferred_element_type=jnp.float32) * inv_rms
        lane = lax.broadcasted_iota(jnp.int32, raw.shape, 1)
        softplus = jnp.maximum(raw, 0.0) + jnp.log1p(jnp.exp(-jnp.abs(raw)))
        gates_ref[at(r), :] = jnp.where(lane < heads, jax.nn.sigmoid(raw), -rate_ref[...] * softplus)
        return carry

    lax.fori_loop(0, CHUNKS, chunk, 0)
    for r in range(CHUNKS):
        for o in range(1, chips):
            across(o, r).wait_send()
            forward(o, r).wait_send()
        beside(r).wait_send()


def project(tokens, weights, w_gates, rates, heads):
    rows, part = tokens.shape
    tp = lax.axis_size("tp")
    others = max(tp // 2 - 1, 1)
    vm = pl.BlockSpec(memory_space=pltpu.VMEM)
    dma = pltpu.SemaphoreType.DMA
    return pl.pallas_call(
        functools.partial(project_kernel, heads),
        out_shape=tuple(
            jax.ShapeDtypeStruct((rows, w.shape[1]), jnp.bfloat16) for w in weights
        )
        + (jax.ShapeDtypeStruct((rows, w_gates.shape[1]), jnp.float32),),
        in_specs=[vm] * (3 + len(weights)),
        out_specs=(vm,) * (1 + len(weights)),
        scratch_shapes=[
            pltpu.VMEM((rows, part * tp), jnp.bfloat16),
            dma((others, CHUNKS)),
            dma((others, CHUNKS)),
            dma((CHUNKS,)),
            dma((CHUNKS,)),
            dma((others, CHUNKS)),
            dma((others, CHUNKS)),
        ],
        compiler_params=pltpu.CompilerParams(
            collective_id=0, has_side_effects=True, vmem_limit_bytes=48 * 1024 * 1024
        ),
        cost_estimate=pl.CostEstimate(
            flops=10_000_000_000, bytes_accessed=20_000_000, transcendentals=0
        ),
        name="gather_project",
    )(tokens, *weights, w_gates, rates)


def middle_kernel(
    heads, width, final_ref, gv_ref, gg_ref, cg_ref, taps_ref, ln_gain_ref, ln_shift_ref,
    outa_ref, outb_ref, dg_ref, gain_ref, mixed_ref, conv_ref,
    padded, filtered, halo_out, halo_in, sums_out, sums_in, near, window_s, sent_s, far_s,
    near_send, near_recv, far_send, far_recv, halo_send, halo_recv, ln_send, ln_recv,
):
    rows = gv_ref.shape[0]
    halo = halo_in.shape[0]
    lanes = padded.shape[2]
    groups = padded.shape[0]
    kernel = taps_ref.shape[0]
    tiles = rows // BLOCK
    sp, place = lax.axis_size("sp"), lax.axis_index("sp")
    tp, me = lax.axis_size("tp"), lax.axis_index("tp")
    reaches = [2]
    while 2 * reaches[-1] < sp:
        reaches.append(2 * reaches[-1])
    distances = [1, 2] + reaches[1:]
    barrier = pltpu.get_barrier_semaphore()
    for step in distances:
        for to in (step, sp - step):
            pl.semaphore_signal(
                barrier, inc=1, device_id={"sp": lax.rem(place + to, sp)}, device_id_type=MESH
            )
    for step in range(1, tp):
        pl.semaphore_signal(
            barrier, inc=1, device_id={"tp": lax.rem(me + step, tp)}, device_id_type=MESH
        )
    pl.semaphore_wait(barrier, 2 * len(distances) + tp - 1)

    def onward(src, dst, send, recv, step):
        return pltpu.make_async_remote_copy(
            src_ref=src,
            dst_ref=dst,
            send_sem=send,
            recv_sem=recv,
            device_id={"sp": lax.rem(place + step, sp)},
            device_id_type=MESH,
        )

    firsts = [
        onward(final_ref, near.at[i], near_send.at[i], near_recv.at[i], i + 1) for i in range(2)
    ]
    for copy in firsts:
        copy.start()

    def at(t):
        return pl.ds(pl.multiple_of(t * BLOCK, BLOCK), BLOCK)

    def unit(t, carry):
        value = gv_ref[at(t), :].astype(jnp.float32)
        units = (value * jax.nn.sigmoid(gg_ref[at(t), :].astype(jnp.float32))).astype(jnp.bfloat16)
        wide = units.astype(jnp.float32)
        for g in range(groups):
            padded[g, pl.ds(pl.multiple_of(t * BLOCK + halo, halo), BLOCK), :] = wide[
                :, g * lanes : (g + 1) * lanes
            ]
        return units

    units = unit(tiles - 1, 0)
    halo_out[...] = units[BLOCK - halo :, :]
    halo_copy = onward(halo_out, halo_in, halo_send.at[0], halo_recv.at[0], 1)
    halo_copy.start()

    def unit_loop(t, carry):
        unit(t, 0)
        return carry

    lax.fori_loop(0, tiles - 1, unit_loop, 0)

    def conv(t, carry):
        first = jnp.zeros((BLOCK, 1), jnp.float32)
        second = jnp.zeros((BLOCK, 1), jnp.float32)
        for g in range(groups):
            total = jnp.zeros((BLOCK, lanes), jnp.float32)
            for j in range(kernel):
                start = t * BLOCK + (halo - kernel + 1 + j)
                tap = taps_ref[j : j + 1, g * lanes : (g + 1) * lanes]
                total = total + padded[g, pl.ds(start, BLOCK), :] * tap
            filtered[g, at(t), :] = total
            first = first + jnp.sum(total, axis=1, keepdims=True)
            second = second + jnp.sum(total * total, axis=1, keepdims=True)
        lane = lax.broadcasted_iota(jnp.int32, (BLOCK, BLOCK), 1)
        sums_out[t] = jnp.where(lane == 0, first, jnp.where(lane == 1, second, 0.0)).T[:8, :]
        return carry

    half = tiles // 2
    lax.fori_loop(1, half, conv, 0)
    for copy in firsts:
        copy.wait()
    for h in range(heads):
        one = jnp.where(place >= 1, near[0, h].astype(jnp.float32), 0.0)
        two = jnp.where(place >= 2, near[1, h].astype(jnp.float32), 0.0)
        moved = mm(one[:, :width], two)
        window_s[h] = jnp.concatenate(
            [moved[:, :width], moved[:, width:] + one[:, width:]], axis=1
        )
        sent_s[0, h] = window_s[h].astype(jnp.bfloat16)

    def step_copy(i):
        return onward(sent_s.at[i], far_s.at[i], far_send.at[i], far_recv.at[i], reaches[i])

    step_copy(0).start()
    lax.fori_loop(half, tiles, conv, 0)
    halo_copy.wait()
    before = jnp.where(place >= 1, halo_in[...].astype(jnp.float32), 0.0)
    for g in range(groups):
        padded[g, :halo, :] = before[:, g * lanes : (g + 1) * lanes]
    conv(0, 0)

    def ln_copy(step):
        return pltpu.make_async_remote_copy(
            src_ref=sums_out,
            dst_ref=sums_in.at[step - 1],
            send_sem=ln_send.at[step - 1],
            recv_sem=ln_recv.at[step - 1],
            device_id={"tp": lax.rem(me + step, tp)},
            device_id_type=MESH,
        )

    for step in range(1, tp):
        ln_copy(step).start()
    for i in range(len(reaches) - 1):
        step_copy(i).wait()
        for h in range(heads):
            earlier = jnp.where(place >= reaches[i], far_s[i, h].astype(jnp.float32), 0.0)
            window = window_s[h]
            moved = mm(window[:, :width], earlier)
            window_s[h] = jnp.concatenate(
                [moved[:, :width], moved[:, width:] + window[:, width:]], axis=1
            )
            sent_s[i + 1, h] = window_s[h].astype(jnp.bfloat16)
        step_copy(i + 1).start()
    for step in range(1, tp):
        ln_copy(step).wait()
    channels = groups * lanes * tp

    def norm(t, carry):
        sums = sums_out[t]
        for step in range(1, tp):
            sums = sums + sums_in[step - 1, t]
        sums = jnp.concatenate([sums, jnp.zeros((BLOCK - 8, BLOCK), jnp.float32)], axis=0).T
        center = sums[:, 0:1] / channels
        variance = jnp.maximum(sums[:, 1:2] / channels - center * center, 0.0)
        scale = lax.rsqrt(variance + TINY_VAR)
        for g in range(groups):
            cut = slice(g * lanes, (g + 1) * lanes)
            normed = (filtered[g, at(t), :] - center) * scale
            normed = normed * ln_gain_ref[:, cut] + ln_shift_ref[:, cut]
            gate = cg_ref[at(t), cut].astype(jnp.float32)
            conv_ref[at(t), cut] = (jax.nn.silu(normed) * jax.nn.silu(gate)).astype(jnp.bfloat16)
        return carry

    lax.fori_loop(0, tiles, norm, 0)
    last = len(reaches) - 1
    step_copy(last).wait()
    carried = []
    for h in range(heads):
        earlier = jnp.where(
            place >= reaches[last], far_s[last, h, :, width:].astype(jnp.float32), 0.0
        )
        window = window_s[h]
        carried.append((mm(window[:, :width], earlier) + window[:, width:]).astype(jnp.bfloat16))

    def one_tile(t, carry):
        for h in range(heads):
            cut = slice(h * width, (h + 1) * width)
            result = outb_ref[h, at(t), :] + mm(outa_ref[h, at(t), :], carried[h])
            result = result * lax.rsqrt(
                jnp.mean(result * result, axis=-1, keepdims=True) + TINY_NORM
            )
            gate = dg_ref[at(t), cut].astype(jnp.float32)
            mixed_ref[at(t), cut] = (result * gain_ref[...] * jax.nn.silu(gate)).astype(
                jnp.bfloat16
            )
        return carry

    lax.fori_loop(0, tiles, one_tile, 0)


def middle(final, glu_value, glu_gate, conv_gate, taps, ln_gain, ln_shift, outa, outb, gate, gain):
    heads, width = final.shape[0], final.shape[1]
    rows, channels = glu_value.shape
    kernel = taps.shape[0]
    halo = (kernel - 1 + 31) // 32 * 32
    lanes = min(channels, 128)
    groups = channels // lanes
    sp, tp = lax.axis_size("sp"), lax.axis_size("tp")
    steps = 1
    while 2 ** (steps + 1) < sp:
        steps += 1
    vm = pl.BlockSpec(memory_space=pltpu.VMEM)
    dma = pltpu.SemaphoreType.DMA
    tiles = rows // BLOCK
    pair = (heads, width, 2 * width)
    return pl.pallas_call(
        functools.partial(middle_kernel, heads, width),
        out_shape=(
            jax.ShapeDtypeStruct((rows, heads * width), jnp.bfloat16),
            jax.ShapeDtypeStruct((rows, channels), jnp.bfloat16),
        ),
        in_specs=[vm] * 11,
        out_specs=(vm, vm),
        scratch_shapes=[
            pltpu.VMEM((groups, halo + rows, lanes), jnp.float32),
            pltpu.VMEM((groups, rows, lanes), jnp.float32),
            pltpu.VMEM((halo, channels), jnp.bfloat16),
            pltpu.VMEM((halo, channels), jnp.bfloat16),
            pltpu.VMEM((tiles, 8, BLOCK), jnp.float32),
            pltpu.VMEM((tp - 1, tiles, 8, BLOCK), jnp.float32),
            pltpu.VMEM((2,) + pair, jnp.bfloat16),
            pltpu.VMEM(pair, jnp.float32),
            pltpu.VMEM((steps,) + pair, jnp.bfloat16),
            pltpu.VMEM((steps,) + pair, jnp.bfloat16),
            dma((2,)),
            dma((2,)),
            dma((steps,)),
            dma((steps,)),
            dma((1,)),
            dma((1,)),
            dma((tp - 1,)),
            dma((tp - 1,)),
        ],
        compiler_params=pltpu.CompilerParams(
            collective_id=2, has_side_effects=True, vmem_limit_bytes=40 * 1024 * 1024
        ),
        cost_estimate=pl.CostEstimate(
            flops=10_000_000_000, bytes_accessed=20_000_000, transcendentals=0
        ),
        name="exchange_middle",
    )(final, glu_value, glu_gate, conv_gate, taps, ln_gain, ln_shift, outa, outb, gate, gain)


def output_kernel(
    dm_ref, cm_ref, wd_ref, wc_ref, out_ref,
    beside_out, beside_in, across_out, across_in, b_send, b_recv, y_send, y_recv,
):
    chips, me, core, chip, sibling = sharded_place()
    rows = out_ref.shape[0]
    width = out_ref.shape[1] // CUTS

    def cols(n):
        return pl.ds(pl.multiple_of(n * width, width), width)

    def partial(target, n):
        at = pl.ds(pl.multiple_of(target * rows, rows), rows)
        summed = jnp.dot(dm_ref[at, :], wd_ref[:, cols(n)], preferred_element_type=jnp.float32)
        return summed + jnp.dot(
            cm_ref[at, :], wc_ref[:, cols(n)], preferred_element_type=jnp.float32
        )

    def beside(o, n):
        return pltpu.make_async_remote_copy(
            src_ref=beside_out.at[o, n],
            dst_ref=beside_in.at[o, n],
            send_sem=b_send.at[o, n],
            recv_sem=b_recv.at[o, n],
            device_id={"tp": sibling},
            device_id_type=MESH,
        )

    def across(o, n):
        there = lax.rem(chip + o, chips) * 2 + core
        return pltpu.make_async_remote_copy(
            src_ref=across_out.at[o - 1, n],
            dst_ref=across_in.at[o - 1, n],
            send_sem=y_send.at[o - 1, n],
            recv_sem=y_recv.at[o - 1, n],
            device_id={"tp": there},
            device_id_type=MESH,
        )

    greet(chips, core, chip, sibling)
    order = list(range(1, chips)) + [0]
    for o in order:
        their_chip = lax.rem(chip + o, chips) * 2

        def give(n, carry, o=o, their_chip=their_chip):
            beside_out[o, n] = partial(their_chip + 1 - core, n).astype(jnp.bfloat16)
            beside(o, n).start()
            return carry

        def keep(n, carry, o=o, their_chip=their_chip):
            mine = partial(their_chip + core, n)
            beside(o, n).wait_recv()
            mine = mine + beside_in[o, n].astype(jnp.float32)
            across_out[o - 1, n] = mine.astype(jnp.bfloat16)
            across(o, n).start()
            return carry

        if o != 0:

            def both(n, carry, give=give, keep=keep):
                @pl.when(n + 1 < CUTS)
                def _():
                    give(n + 1, 0)

                return keep(n, carry)

            give(0, 0)
            lax.fori_loop(0, CUTS, both, 0)
        else:
            lax.fori_loop(0, CUTS, give, 0)

    def close(n, carry):
        mine = partial(me, n)
        beside(0, n).wait_recv()
        mine = mine + beside_in[0, n].astype(jnp.float32)
        for o in range(1, chips):
            across(o, n).wait_recv()
            mine = mine + across_in[o - 1, n].astype(jnp.float32)
        out_ref[:, cols(n)] = mine.astype(jnp.bfloat16)
        return carry

    lax.fori_loop(0, CUTS, close, 0)

    def drain(n, carry):
        for o in range(chips):
            beside(o, n).wait_send()
        for o in range(1, chips):
            across(o, n).wait_send()
        return carry

    lax.fori_loop(0, CUTS, drain, 0)


def output_projection(delta_mixed, conv_mixed, out_delta, out_conv):
    tp = lax.axis_size("tp")
    chips = tp // 2
    others = max(chips - 1, 1)
    rows = delta_mixed.shape[0] // tp
    width = out_delta.shape[1]
    cut = width // CUTS
    vm = pl.BlockSpec(memory_space=pltpu.VMEM)
    dma = pltpu.SemaphoreType.DMA
    return pl.pallas_call(
        output_kernel,
        out_shape=jax.ShapeDtypeStruct((rows, width), jnp.bfloat16),
        in_specs=[vm] * 4,
        out_specs=vm,
        scratch_shapes=[
            pltpu.VMEM((chips, CUTS, rows, cut), jnp.bfloat16),
            pltpu.VMEM((chips, CUTS, rows, cut), jnp.bfloat16),
            pltpu.VMEM((others, CUTS, rows, cut), jnp.bfloat16),
            pltpu.VMEM((others, CUTS, rows, cut), jnp.bfloat16),
            dma((chips, CUTS)),
            dma((chips, CUTS)),
            dma((others, CUTS)),
            dma((others, CUTS)),
        ],
        compiler_params=pltpu.CompilerParams(
            collective_id=1, has_side_effects=True, vmem_limit_bytes=48 * 1024 * 1024
        ),
        cost_estimate=pl.CostEstimate(
            flops=10_000_000_000, bytes_accessed=20_000_000, transcendentals=0
        ),
        name="output_scatter",
    )(delta_mixed, conv_mixed, out_delta, out_conv)


def local(
    tokens,
    w_query,
    w_key,
    w_value,
    w_delta_gate,
    w_glu_value,
    w_glu_gate,
    w_conv_gate,
    w_beta,
    w_decay,
    decay_log,
    head_gain,
    conv_taps,
    ln_gain,
    ln_shift,
    out_delta,
    out_conv,
):
    head_size = head_gain.shape[0]
    heads_here = w_query.shape[1] // head_size
    first_head = lax.axis_index("tp") * heads_here
    rates = jnp.exp(lax.dynamic_slice_in_dim(decay_log, first_head, heads_here, 0))
    fill = head_size - 2 * heads_here
    rates = jnp.concatenate(
        [jnp.zeros((heads_here,), jnp.float32), rates, jnp.zeros((fill,), jnp.float32)]
    )[None, :]
    w_gates = jnp.concatenate(
        [
            lax.dynamic_slice_in_dim(w_beta, first_head, heads_here, 1),
            lax.dynamic_slice_in_dim(w_decay, first_head, heads_here, 1),
            jnp.zeros((w_beta.shape[0], fill), jnp.bfloat16),
        ],
        axis=1,
    )
    weights = (w_query, w_key, w_value, w_delta_gate, w_glu_value, w_glu_gate, w_conv_gate)
    (
        query_raw,
        key_raw,
        value_raw,
        delta_gate_raw,
        glu_value_raw,
        glu_gate_raw,
        conv_gate_raw,
        gates,
    ) = project(tokens, weights, w_gates, rates, heads_here)
    outa, outb, final = delta_rule(
        query_raw, key_raw, value_raw, gates, heads_here, head_size
    )
    delta_mixed, conv_mixed = middle(
        final,
        glu_value_raw,
        glu_gate_raw,
        conv_gate_raw,
        conv_taps.astype(jnp.float32),
        ln_gain[None, :],
        ln_shift[None, :],
        outa,
        outb,
        delta_gate_raw,
        head_gain[None, :],
    )
    return output_projection(delta_mixed, conv_mixed, out_delta, out_conv)


def solution(mesh):
    return jax.shard_map(
        local,
        mesh=mesh,
        in_specs=(
            P("sp", "tp"),
            P(None, "tp"),
            P(None, "tp"),
            P(None, "tp"),
            P(None, "tp"),
            P(None, "tp"),
            P(None, "tp"),
            P(None, "tp"),
            P(),
            P(),
            P(),
            P(),
            P(None, "tp"),
            P("tp"),
            P("tp"),
            P("tp", None),
            P("tp", None),
        ),
        out_specs=P(("sp", "tp"), None),
        check_vma=False,
    )
```

```python
import functools

import jax
import jax.numpy as jnp
from jax import lax
from jax.experimental import pallas as pl
from jax.experimental.pallas import tpu as pltpu
from jax.sharding import PartitionSpec as P

BLOCK = 128
CHUNKS = 8
CUTS = 8


TINY_NORM = 1e-06
TINY_VAR = 1e-05
HIGHEST = lax.Precision.HIGHEST


def nt(a, b):
    return lax.dot_general(a, b, (((1,), (1,)), ((), ())), preferred_element_type=jnp.float32)


def mm(a, b):
    return jnp.dot(
        a.astype(jnp.bfloat16), b.astype(jnp.bfloat16), preferred_element_type=jnp.float32
    )


def delta_kernel(
    heads, width, q_ref, k_ref, v_ref, g_ref, outa_ref, outb_ref, final_ref,
    lhs_s, corr_s, score_s, wt_s, tail_s, state_ref,
):
    rows = q_ref.shape[0]
    blocks = rows // BLOCK
    row_id = lax.broadcasted_iota(jnp.int32, (BLOCK, BLOCK), 0)
    col_id = lax.broadcasted_iota(jnp.int32, (BLOCK, BLOCK), 1)
    causal = row_id >= col_id
    strict = row_id > col_id
    differ = row_id ^ col_id
    eye = jnp.where(row_id == col_id, 1.0, 0.0)
    tril = jnp.where(causal, 1.0, 0.0)

    def prepare(c):
        at = pl.ds(pl.multiple_of(c * BLOCK, BLOCK), BLOCK)
        gates = g_ref[at, :]
        sums = jnp.dot(tril, gates, precision=HIGHEST, preferred_element_type=jnp.float32)
        chains = []
        for h in range(heads):
            lanes = slice(h * width, (h + 1) * width)
            k, q = k_ref[at, lanes], q_ref[at, lanes]
            v = v_ref[at, lanes].astype(jnp.float32)
            kf, qf = k.astype(jnp.float32), q.astype(jnp.float32)
            ik = lax.rsqrt(jnp.sum(kf * kf, axis=-1, keepdims=True) + TINY_NORM)
            iq = lax.rsqrt(jnp.sum(qf * qf, axis=-1, keepdims=True) + TINY_NORM)
            iq = iq * width ** (-0.5)
            beta = gates[:, h : h + 1]
            log_sum = sums[:, heads + h : heads + h + 1]
            log_full = jnp.broadcast_to(log_sum, (BLOCK, BLOCK))
            spread = log_full - log_full.T
            damp = jnp.where(causal, jnp.exp(jnp.where(causal, spread, 0.0)), 0.0)
            damp = damp * jnp.broadcast_to(ik, (BLOCK, BLOCK)).T
            lower = jnp.where(strict, nt(k, k) * damp * (beta * ik), 0.0)
            score_s[h, at, :] = (nt(q, k) * damp * iq).astype(jnp.bfloat16)
            grow = jnp.exp(log_sum)
            right = jnp.concatenate([v * beta, kf * (beta * ik * grow)], axis=1)
            tail = log_full[BLOCK - 1 : BLOCK, :]
            weighted = kf * (ik * jnp.exp(tail[:, :1] - log_sum))
            wt_s[h, c] = weighted.T.astype(jnp.bfloat16)
            tail_s[h, c] = jnp.broadcast_to(jnp.exp(tail), (8, BLOCK))
            lhs_s[h, c, BLOCK:, :] = (qf * (iq * grow)).astype(jnp.bfloat16)
            chains.append([h, lower, right, eye - jnp.where(differ == 1, lower, 0.0)])
        return at, c, chains

    def pair(p, carry):
        prepared = [prepare(p * 2 + i) for i in range(2)]
        size = 2
        while size < BLOCK:
            level = (differ >= size) & (differ < 2 * size)
            parts = [
                [mm(jnp.where(level, ch[1], 0.0), ch[3]) for ch in item[2]] for item in prepared
            ]
            for item, part in zip(prepared, parts):
                for ch, moved in zip(item[2], part):
                    ch[3] = ch[3] - mm(ch[3], moved)
            size *= 2
        for at, c, chains in prepared:
            for h, lower, right, inverse in chains:
                solved = mm(inverse, right)
                corr_s[h, at, :] = solved[:, :width]
                lhs_s[h, c, :BLOCK, :] = solved[:, width:].astype(jnp.bfloat16)
        return carry

    lax.fori_loop(0, blocks // 2, pair, 0)
    for h in range(heads):
        state_ref[h] = jnp.concatenate([eye, jnp.zeros((width, width), jnp.float32)], axis=1)

    def advance(c, carry):
        at = pl.ds(pl.multiple_of(c * BLOCK, BLOCK), BLOCK)
        boths = [mm(lhs_s[h, c], state_ref[h]) for h in range(heads)]
        fresh = []
        for h in range(heads):
            first = boths[h][:BLOCK]
            fresh.append(
                jnp.concatenate(
                    [-first[:, :width], corr_s[h, at, :] - first[:, width:]], axis=1
                ).astype(jnp.bfloat16)
            )
        for h in range(heads):
            decay = tail_s[h, c][:1, :]
            decay = jnp.concatenate([decay, decay], axis=1)
            state_ref[h] = state_ref[h] * decay + mm(wt_s[h, c], fresh[h])
        for h in range(heads):
            out = boths[h][BLOCK:] + mm(score_s[h, at, :], fresh[h])
            outa_ref[h, at, :] = out[:, :width].astype(jnp.bfloat16)
            outb_ref[h, at, :] = out[:, width:]
        return carry

    lax.fori_loop(0, blocks, advance, 0)
    final_ref[...] = state_ref[...].astype(jnp.bfloat16)


def delta_rule(query_raw, key_raw, value_raw, gates, heads, width):
    rows = query_raw.shape[0]
    blocks = rows // BLOCK
    vm = pl.BlockSpec(memory_space=pltpu.VMEM)
    return pl.pallas_call(
        functools.partial(delta_kernel, heads, width),
        out_shape=(
            jax.ShapeDtypeStruct((heads, rows, width), jnp.bfloat16),
            jax.ShapeDtypeStruct((heads, rows, width), jnp.float32),
            jax.ShapeDtypeStruct((heads, width, 2 * width), jnp.bfloat16),
        ),
        in_specs=[vm] * 4,
        out_specs=(vm, vm, vm),
        scratch_shapes=[
            pltpu.VMEM((heads, blocks, 2 * BLOCK, width), jnp.bfloat16),
            pltpu.VMEM((heads, rows, width), jnp.float32),
            pltpu.VMEM((heads, rows, BLOCK), jnp.bfloat16),
            pltpu.VMEM((heads, blocks, width, BLOCK), jnp.bfloat16),
            pltpu.VMEM((heads, blocks, 8, BLOCK), jnp.float32),
            pltpu.VMEM((heads, width, 2 * width), jnp.float32),
        ],
        compiler_params=pltpu.CompilerParams(
            vmem_limit_bytes=40 * 1024 * 1024
        ),
        cost_estimate=pl.CostEstimate(
            flops=10_000_000_000, bytes_accessed=4_000_000, transcendentals=0
        ),
        name="delta_rule",
    )(query_raw, key_raw, value_raw, gates)


MESH = pl.DeviceIdType.MESH


def sharded_place():
    tp = lax.axis_size("tp")
    me = lax.axis_index("tp")
    core = lax.rem(me, 2)
    return tp // 2, me, core, me // 2, me + 1 - 2 * core


def greet(chips, core, chip, sibling):
    barrier = pltpu.get_barrier_semaphore()
    pl.semaphore_signal(barrier, inc=1, device_id={"tp": sibling}, device_id_type=MESH)
    for o in range(1, chips):
        there = lax.rem(chip + o, chips) * 2 + core
        pl.semaphore_signal(barrier, inc=1, device_id={"tp": there}, device_id_type=MESH)
    pl.semaphore_wait(barrier, chips)


def project_kernel(heads, *refs):
    count = 7
    tok_ref, far_refs, wg_ref, rate_ref = refs[0], refs[1 : 1 + count], refs[8], refs[9]
    out_refs, gates_ref = refs[10 : 10 + count], refs[17]
    full, y_send, y_recv, own_send, own_recv, fwd_send, fwd_recv, w_sem = refs[18:26]
    w_refs = refs[26:]
    rows, part = tok_ref.shape
    step = rows // CHUNKS
    chips, me, core, chip, sibling = sharded_place()

    def columns(owner):
        return pl.ds(pl.multiple_of(owner * part, part), part)

    def at(r):
        return pl.ds(pl.multiple_of(r * step, step), step)

    def across(o, r):
        there = lax.rem(chip + o, chips) * 2 + core
        return pltpu.make_async_remote_copy(
            src_ref=tok_ref.at[at(r), :],
            dst_ref=full.at[at(r), columns(me)],
            send_sem=y_send.at[o - 1, r],
            recv_sem=y_recv.at[o - 1, r],
            device_id={"tp": there},
            device_id_type=MESH,
        )

    def beside(r):
        return pltpu.make_async_remote_copy(
            src_ref=tok_ref.at[at(r), :],
            dst_ref=full.at[at(r), columns(me)],
            send_sem=own_send.at[r],
            recv_sem=own_recv.at[r],
            device_id={"tp": sibling},
            device_id_type=MESH,
        )

    def forward(o, r):
        owner = lax.rem(chip - o + chips, chips) * 2 + core
        block = full.at[at(r), columns(owner)]
        return pltpu.make_async_remote_copy(
            src_ref=block,
            dst_ref=block,
            send_sem=fwd_send.at[o - 1, r],
            recv_sem=fwd_recv.at[o - 1, r],
            device_id={"tp": sibling},
            device_id_type=MESH,
        )

    greet(chips, core, chip, sibling)
    for r in range(CHUNKS):
        for o in range(1, chips):
            across(o, r).start()
    loads = [
        pltpu.make_async_copy(far, w_ref, w_sem.at[i])
        for i, (far, w_ref) in enumerate(zip(far_refs, w_refs))
    ]
    for load in loads:
        load.start()
    for r in range(CHUNKS):
        beside(r).start()
    full[:, columns(me)] = tok_ref[...]

    def chunk(first, pieces, carry):
        for i in range(pieces):
            for o in range(1, chips):
                across(o, first + i).wait_recv()
                forward(o, first + i).start()
        for i in range(pieces):
            beside(first + i).wait_recv()
            for o in range(1, chips):
                forward(o, first + i).wait_recv()
        size = step * pieces
        here = pl.ds(pl.multiple_of(first * step, step), size)
        squares = jnp.zeros((size, 1), jnp.float32)
        for b in range(2 * chips):
            piece = full[here, b * part : (b + 1) * part].astype(jnp.float32)
            squares = squares + jnp.sum(piece * piece, axis=1, keepdims=True)
        inv_rms = lax.rsqrt(squares / (part * 2 * chips) + TINY_NORM)
        for w_ref, out_ref in zip(w_refs, out_refs):
            summed = jnp.dot(full[here, :], w_ref[...], preferred_element_type=jnp.float32)
            out_ref[here, :] = (summed * inv_rms).astype(jnp.bfloat16)
        raw = jnp.dot(full[here, :], wg_ref[...], preferred_element_type=jnp.float32) * inv_rms
        lane = lax.broadcasted_iota(jnp.int32, raw.shape, 1)
        softplus = jnp.maximum(raw, 0.0) + jnp.log1p(jnp.exp(-jnp.abs(raw)))
        gates_ref[here, :] = jnp.where(lane < heads, jax.nn.sigmoid(raw), -rate_ref[...] * softplus)
        return carry

    for load in loads:
        load.wait()
    paired = CHUNKS // 2 - 1
    lax.fori_loop(0, paired, lambda r, carry: chunk(2 * r, 2, carry), 0)
    lax.fori_loop(2 * paired, CHUNKS, lambda r, carry: chunk(r, 1, carry), 0)
    for r in range(CHUNKS):
        for o in range(1, chips):
            across(o, r).wait_send()
            forward(o, r).wait_send()
        beside(r).wait_send()


def project(tokens, weights, w_gates, rates, heads):
    rows, part = tokens.shape
    tp = lax.axis_size("tp")
    others = max(tp // 2 - 1, 1)
    vm = pl.BlockSpec(memory_space=pltpu.VMEM)
    dma = pltpu.SemaphoreType.DMA
    return pl.pallas_call(
        functools.partial(project_kernel, heads),
        out_shape=tuple(
            jax.ShapeDtypeStruct((rows, w.shape[1]), jnp.bfloat16) for w in weights
        )
        + (jax.ShapeDtypeStruct((rows, w_gates.shape[1]), jnp.float32),),
        in_specs=[vm] + [pl.BlockSpec(memory_space=pl.ANY)] * len(weights) + [vm] * 2,
        out_specs=(vm,) * (1 + len(weights)),
        scratch_shapes=[
            pltpu.VMEM((rows, part * tp), jnp.bfloat16),
            dma((others, CHUNKS)),
            dma((others, CHUNKS)),
            dma((CHUNKS,)),
            dma((CHUNKS,)),
            dma((others, CHUNKS)),
            dma((others, CHUNKS)),
            dma((len(weights),)),
        ]
        + [pltpu.VMEM(w.shape, w.dtype) for w in weights],
        compiler_params=pltpu.CompilerParams(
            collective_id=0, has_side_effects=True, vmem_limit_bytes=48 * 1024 * 1024
        ),
        cost_estimate=pl.CostEstimate(
            flops=10_000_000_000, bytes_accessed=20_000_000, transcendentals=0
        ),
        name="gather_project",
    )(tokens, *weights, w_gates, rates)


def middle_kernel(
    heads, width, final_ref, gv_ref, gg_ref, cg_ref, taps_ref, ln_gain_ref, ln_shift_ref,
    outa_ref, outb_ref, dg_ref, gain_ref, mixed_ref, conv_ref,
    padded, filtered, halo_out, halo_in, sums_out, sums_in, near, window_s, sent_s, far_s,
    near_send, near_recv, far_send, far_recv, halo_send, halo_recv, ln_send, ln_recv,
):
    rows = gv_ref.shape[0]
    halo = halo_in.shape[0]
    lanes = padded.shape[2]
    groups = padded.shape[0]
    kernel = taps_ref.shape[0]
    tiles = rows // BLOCK
    sp, place = lax.axis_size("sp"), lax.axis_index("sp")
    tp, me = lax.axis_size("tp"), lax.axis_index("tp")
    reaches = [2]
    while 2 * reaches[-1] < sp:
        reaches.append(2 * reaches[-1])
    distances = [1, 2] + reaches[1:]
    barrier = pltpu.get_barrier_semaphore()
    for step in distances:
        for to in (step, sp - step):
            pl.semaphore_signal(
                barrier, inc=1, device_id={"sp": lax.rem(place + to, sp)}, device_id_type=MESH
            )
    for step in range(1, tp):
        pl.semaphore_signal(
            barrier, inc=1, device_id={"tp": lax.rem(me + step, tp)}, device_id_type=MESH
        )
    pl.semaphore_wait(barrier, 2 * len(distances) + tp - 1)

    def onward(src, dst, send, recv, step):
        return pltpu.make_async_remote_copy(
            src_ref=src,
            dst_ref=dst,
            send_sem=send,
            recv_sem=recv,
            device_id={"sp": lax.rem(place + step, sp)},
            device_id_type=MESH,
        )

    firsts = [
        onward(final_ref, near.at[i], near_send.at[i], near_recv.at[i], i + 1) for i in range(2)
    ]
    for copy in firsts:
        copy.start()

    def at(t):
        return pl.ds(pl.multiple_of(t * BLOCK, BLOCK), BLOCK)

    def unit(t, carry):
        value = gv_ref[at(t), :].astype(jnp.float32)
        units = (value * jax.nn.sigmoid(gg_ref[at(t), :].astype(jnp.float32))).astype(jnp.bfloat16)
        wide = units.astype(jnp.float32)
        for g in range(groups):
            padded[g, pl.ds(pl.multiple_of(t * BLOCK + halo, halo), BLOCK), :] = wide[
                :, g * lanes : (g + 1) * lanes
            ]
        return units

    units = unit(tiles - 1, 0)
    halo_out[...] = units[BLOCK - halo :, :]
    halo_copy = onward(halo_out, halo_in, halo_send.at[0], halo_recv.at[0], 1)
    halo_copy.start()

    def unit_loop(t, carry):
        unit(t, 0)
        return carry

    lax.fori_loop(0, tiles - 1, unit_loop, 0)

    def conv(t, carry):
        first = jnp.zeros((BLOCK, 1), jnp.float32)
        second = jnp.zeros((BLOCK, 1), jnp.float32)
        for g in range(groups):
            total = jnp.zeros((BLOCK, lanes), jnp.float32)
            for j in range(kernel):
                start = t * BLOCK + (halo - kernel + 1 + j)
                tap = taps_ref[j : j + 1, g * lanes : (g + 1) * lanes]
                total = total + padded[g, pl.ds(start, BLOCK), :] * tap
            filtered[g, at(t), :] = total
            first = first + jnp.sum(total, axis=1, keepdims=True)
            second = second + jnp.sum(total * total, axis=1, keepdims=True)
        lane = lax.broadcasted_iota(jnp.int32, (BLOCK, BLOCK), 1)
        sums_out[t] = jnp.where(lane == 0, first, jnp.where(lane == 1, second, 0.0)).T[:8, :]
        return carry

    half = tiles // 2
    lax.fori_loop(1, half, conv, 0)
    for copy in firsts:
        copy.wait()
    for h in range(heads):
        one = jnp.where(place >= 1, near[0, h].astype(jnp.float32), 0.0)
        two = jnp.where(place >= 2, near[1, h].astype(jnp.float32), 0.0)
        moved = mm(one[:, :width], two)
        window_s[h] = jnp.concatenate(
            [moved[:, :width], moved[:, width:] + one[:, width:]], axis=1
        )
        sent_s[0, h] = window_s[h].astype(jnp.bfloat16)

    def step_copy(i):
        return onward(sent_s.at[i], far_s.at[i], far_send.at[i], far_recv.at[i], reaches[i])

    step_copy(0).start()
    lax.fori_loop(half, tiles, conv, 0)
    halo_copy.wait()
    before = jnp.where(place >= 1, halo_in[...].astype(jnp.float32), 0.0)
    for g in range(groups):
        padded[g, :halo, :] = before[:, g * lanes : (g + 1) * lanes]
    conv(0, 0)

    def ln_copy(step):
        return pltpu.make_async_remote_copy(
            src_ref=sums_out,
            dst_ref=sums_in.at[step - 1],
            send_sem=ln_send.at[step - 1],
            recv_sem=ln_recv.at[step - 1],
            device_id={"tp": lax.rem(me + step, tp)},
            device_id_type=MESH,
        )

    for step in range(1, tp):
        ln_copy(step).start()
    for i in range(len(reaches) - 1):
        step_copy(i).wait()
        for h in range(heads):
            earlier = jnp.where(place >= reaches[i], far_s[i, h].astype(jnp.float32), 0.0)
            window = window_s[h]
            moved = mm(window[:, :width], earlier)
            window_s[h] = jnp.concatenate(
                [moved[:, :width], moved[:, width:] + window[:, width:]], axis=1
            )
            sent_s[i + 1, h] = window_s[h].astype(jnp.bfloat16)
        step_copy(i + 1).start()
    for step in range(1, tp):
        ln_copy(step).wait()
    channels = groups * lanes * tp

    def norm(t, carry):
        sums = sums_out[t]
        for step in range(1, tp):
            sums = sums + sums_in[step - 1, t]
        sums = jnp.concatenate([sums, jnp.zeros((BLOCK - 8, BLOCK), jnp.float32)], axis=0).T
        center = sums[:, 0:1] / channels
        variance = jnp.maximum(sums[:, 1:2] / channels - center * center, 0.0)
        scale = lax.rsqrt(variance + TINY_VAR)
        for g in range(groups):
            cut = slice(g * lanes, (g + 1) * lanes)
            normed = (filtered[g, at(t), :] - center) * scale
            normed = normed * ln_gain_ref[:, cut] + ln_shift_ref[:, cut]
            gate = cg_ref[at(t), cut].astype(jnp.float32)
            conv_ref[at(t), cut] = (jax.nn.silu(normed) * jax.nn.silu(gate)).astype(jnp.bfloat16)
        return carry

    lax.fori_loop(0, tiles, norm, 0)
    last = len(reaches) - 1
    step_copy(last).wait()
    carried = []
    for h in range(heads):
        earlier = jnp.where(
            place >= reaches[last], far_s[last, h, :, width:].astype(jnp.float32), 0.0
        )
        window = window_s[h]
        carried.append((mm(window[:, :width], earlier) + window[:, width:]).astype(jnp.bfloat16))

    def one_tile(t, carry):
        for h in range(heads):
            cut = slice(h * width, (h + 1) * width)
            result = outb_ref[h, at(t), :] + mm(outa_ref[h, at(t), :], carried[h])
            result = result * lax.rsqrt(
                jnp.mean(result * result, axis=-1, keepdims=True) + TINY_NORM
            )
            gate = dg_ref[at(t), cut].astype(jnp.float32)
            mixed_ref[at(t), cut] = (result * gain_ref[...] * jax.nn.silu(gate)).astype(
                jnp.bfloat16
            )
        return carry

    lax.fori_loop(0, tiles, one_tile, 0)


def middle(final, glu_value, glu_gate, conv_gate, taps, ln_gain, ln_shift, outa, outb, gate, gain):
    heads, width = final.shape[0], final.shape[1]
    rows, channels = glu_value.shape
    kernel = taps.shape[0]
    halo = (kernel - 1 + 31) // 32 * 32
    lanes = min(channels, 128)
    groups = channels // lanes
    sp, tp = lax.axis_size("sp"), lax.axis_size("tp")
    steps = 1
    while 2 ** (steps + 1) < sp:
        steps += 1
    vm = pl.BlockSpec(memory_space=pltpu.VMEM)
    dma = pltpu.SemaphoreType.DMA
    tiles = rows // BLOCK
    pair = (heads, width, 2 * width)
    return pl.pallas_call(
        functools.partial(middle_kernel, heads, width),
        out_shape=(
            jax.ShapeDtypeStruct((rows, heads * width), jnp.bfloat16),
            jax.ShapeDtypeStruct((rows, channels), jnp.bfloat16),
        ),
        in_specs=[vm] * 11,
        out_specs=(vm, vm),
        scratch_shapes=[
            pltpu.VMEM((groups, halo + rows, lanes), jnp.float32),
            pltpu.VMEM((groups, rows, lanes), jnp.float32),
            pltpu.VMEM((halo, channels), jnp.bfloat16),
            pltpu.VMEM((halo, channels), jnp.bfloat16),
            pltpu.VMEM((tiles, 8, BLOCK), jnp.float32),
            pltpu.VMEM((tp - 1, tiles, 8, BLOCK), jnp.float32),
            pltpu.VMEM((2,) + pair, jnp.bfloat16),
            pltpu.VMEM(pair, jnp.float32),
            pltpu.VMEM((steps,) + pair, jnp.bfloat16),
            pltpu.VMEM((steps,) + pair, jnp.bfloat16),
            dma((2,)),
            dma((2,)),
            dma((steps,)),
            dma((steps,)),
            dma((1,)),
            dma((1,)),
            dma((tp - 1,)),
            dma((tp - 1,)),
        ],
        compiler_params=pltpu.CompilerParams(
            collective_id=2, has_side_effects=True, vmem_limit_bytes=40 * 1024 * 1024
        ),
        cost_estimate=pl.CostEstimate(
            flops=10_000_000_000, bytes_accessed=20_000_000, transcendentals=0
        ),
        name="exchange_middle",
    )(final, glu_value, glu_gate, conv_gate, taps, ln_gain, ln_shift, outa, outb, gate, gain)


def output_kernel(
    dm_ref, cm_ref, wd_ref, wc_ref, out_ref,
    beside_out, beside_in, across_out, across_in, b_send, b_recv, y_send, y_recv,
):
    chips, me, core, chip, sibling = sharded_place()
    rows = out_ref.shape[0]
    width = out_ref.shape[1] // CUTS

    def cols(n):
        return pl.ds(pl.multiple_of(n * width, width), width)

    def partial(target, n):
        at = pl.ds(pl.multiple_of(target * rows, rows), rows)
        summed = jnp.dot(dm_ref[at, :], wd_ref[:, cols(n)], preferred_element_type=jnp.float32)
        return summed + jnp.dot(
            cm_ref[at, :], wc_ref[:, cols(n)], preferred_element_type=jnp.float32
        )

    def beside(o, n):
        return pltpu.make_async_remote_copy(
            src_ref=beside_out.at[o, n],
            dst_ref=beside_in.at[o, n],
            send_sem=b_send.at[o, n],
            recv_sem=b_recv.at[o, n],
            device_id={"tp": sibling},
            device_id_type=MESH,
        )

    def across(o, n):
        there = lax.rem(chip + o, chips) * 2 + core
        return pltpu.make_async_remote_copy(
            src_ref=across_out.at[o - 1, n],
            dst_ref=across_in.at[o - 1, n],
            send_sem=y_send.at[o - 1, n],
            recv_sem=y_recv.at[o - 1, n],
            device_id={"tp": there},
            device_id_type=MESH,
        )

    greet(chips, core, chip, sibling)
    order = list(range(1, chips)) + [0]
    for o in order:
        their_chip = lax.rem(chip + o, chips) * 2

        def give(n, carry, o=o, their_chip=their_chip):
            beside_out[o, n] = partial(their_chip + 1 - core, n).astype(jnp.bfloat16)
            beside(o, n).start()
            return carry

        def keep(n, carry, o=o, their_chip=their_chip):
            mine = partial(their_chip + core, n)
            beside(o, n).wait_recv()
            mine = mine + beside_in[o, n].astype(jnp.float32)
            across_out[o - 1, n] = mine.astype(jnp.bfloat16)
            across(o, n).start()
            return carry

        if o != 0:

            def both(n, carry, give=give, keep=keep):
                @pl.when(n + 1 < CUTS)
                def _():
                    give(n + 1, 0)

                return keep(n, carry)

            give(0, 0)
            lax.fori_loop(0, CUTS, both, 0)
        else:
            lax.fori_loop(0, CUTS, give, 0)

    def close(n, carry):
        mine = partial(me, n)
        beside(0, n).wait_recv()
        mine = mine + beside_in[0, n].astype(jnp.float32)
        for o in range(1, chips):
            across(o, n).wait_recv()
            mine = mine + across_in[o - 1, n].astype(jnp.float32)
        out_ref[:, cols(n)] = mine.astype(jnp.bfloat16)
        return carry

    lax.fori_loop(0, CUTS, close, 0)

    def drain(n, carry):
        for o in range(chips):
            beside(o, n).wait_send()
        for o in range(1, chips):
            across(o, n).wait_send()
        return carry

    lax.fori_loop(0, CUTS, drain, 0)


def output_projection(delta_mixed, conv_mixed, out_delta, out_conv):
    tp = lax.axis_size("tp")
    chips = tp // 2
    others = max(chips - 1, 1)
    rows = delta_mixed.shape[0] // tp
    width = out_delta.shape[1]
    cut = width // CUTS
    vm = pl.BlockSpec(memory_space=pltpu.VMEM)
    dma = pltpu.SemaphoreType.DMA
    return pl.pallas_call(
        output_kernel,
        out_shape=jax.ShapeDtypeStruct((rows, width), jnp.bfloat16),
        in_specs=[vm] * 4,
        out_specs=vm,
        scratch_shapes=[
            pltpu.VMEM((chips, CUTS, rows, cut), jnp.bfloat16),
            pltpu.VMEM((chips, CUTS, rows, cut), jnp.bfloat16),
            pltpu.VMEM((others, CUTS, rows, cut), jnp.bfloat16),
            pltpu.VMEM((others, CUTS, rows, cut), jnp.bfloat16),
            dma((chips, CUTS)),
            dma((chips, CUTS)),
            dma((others, CUTS)),
            dma((others, CUTS)),
        ],
        compiler_params=pltpu.CompilerParams(
            collective_id=1, has_side_effects=True, vmem_limit_bytes=48 * 1024 * 1024
        ),
        cost_estimate=pl.CostEstimate(
            flops=10_000_000_000, bytes_accessed=20_000_000, transcendentals=0
        ),
        name="output_scatter",
    )(delta_mixed, conv_mixed, out_delta, out_conv)


def local(
    tokens,
    w_query,
    w_key,
    w_value,
    w_delta_gate,
    w_glu_value,
    w_glu_gate,
    w_conv_gate,
    w_beta,
    w_decay,
    decay_log,
    head_gain,
    conv_taps,
    ln_gain,
    ln_shift,
    out_delta,
    out_conv,
):
    head_size = head_gain.shape[0]
    heads_here = w_query.shape[1] // head_size
    first_head = lax.axis_index("tp") * heads_here
    rates = jnp.exp(lax.dynamic_slice_in_dim(decay_log, first_head, heads_here, 0))
    fill = head_size - 2 * heads_here
    rates = jnp.concatenate(
        [jnp.zeros((heads_here,), jnp.float32), rates, jnp.zeros((fill,), jnp.float32)]
    )[None, :]
    w_gates = jnp.concatenate(
        [
            lax.dynamic_slice_in_dim(w_beta, first_head, heads_here, 1),
            lax.dynamic_slice_in_dim(w_decay, first_head, heads_here, 1),
            jnp.zeros((w_beta.shape[0], fill), jnp.bfloat16),
        ],
        axis=1,
    )
    weights = (w_query, w_key, w_value, w_delta_gate, w_glu_value, w_glu_gate, w_conv_gate)
    (
        query_raw,
        key_raw,
        value_raw,
        delta_gate_raw,
        glu_value_raw,
        glu_gate_raw,
        conv_gate_raw,
        gates,
    ) = project(tokens, weights, w_gates, rates, heads_here)
    outa, outb, final = delta_rule(
        query_raw, key_raw, value_raw, gates, heads_here, head_size
    )
    delta_mixed, conv_mixed = middle(
        final,
        glu_value_raw,
        glu_gate_raw,
        conv_gate_raw,
        conv_taps.astype(jnp.float32),
        ln_gain[None, :],
        ln_shift[None, :],
        outa,
        outb,
        delta_gate_raw,
        head_gain[None, :],
    )
    return output_projection(delta_mixed, conv_mixed, out_delta, out_conv)


def solution(mesh):
    return jax.shard_map(
        local,
        mesh=mesh,
        in_specs=(
            P("sp", "tp"),
            P(None, "tp"),
            P(None, "tp"),
            P(None, "tp"),
            P(None, "tp"),
            P(None, "tp"),
            P(None, "tp"),
            P(None, "tp"),
            P(),
            P(),
            P(),
            P(),
            P(None, "tp"),
            P("tp"),
            P("tp"),
            P("tp", None),
            P("tp", None),
        ),
        out_specs=P(("sp", "tp"), None),
        check_vma=False,
    )
```

```python
import functools

import jax
import jax.numpy as jnp
from jax import lax
from jax.experimental import pallas as pl
from jax.experimental.pallas import tpu as pltpu
from jax.sharding import PartitionSpec as P

BLOCK = 128
CHUNKS = 8
TOGETHER = 4
CUTS = 8


TINY_NORM = 1e-06
TINY_VAR = 1e-05
HIGHEST = lax.Precision.HIGHEST


def nt(a, b):
    return lax.dot_general(a, b, (((1,), (1,)), ((), ())), preferred_element_type=jnp.float32)


def mm(a, b):
    return jnp.dot(
        a.astype(jnp.bfloat16), b.astype(jnp.bfloat16), preferred_element_type=jnp.float32
    )


def delta_kernel(
    heads, width, q_ref, k_ref, v_ref, g_ref, outa_ref, outb_ref, final_ref,
    lhs_s, corr_s, score_s, wt_s, tail_s, state_ref,
):
    rows = q_ref.shape[0]
    blocks = rows // BLOCK
    row_id = lax.broadcasted_iota(jnp.int32, (BLOCK, BLOCK), 0)
    col_id = lax.broadcasted_iota(jnp.int32, (BLOCK, BLOCK), 1)
    causal = row_id >= col_id
    strict = row_id > col_id
    differ = row_id ^ col_id
    eye = jnp.where(row_id == col_id, 1.0, 0.0)
    tril = jnp.where(causal, 1.0, 0.0)

    def prepare(c):
        at = pl.ds(pl.multiple_of(c * BLOCK, BLOCK), BLOCK)
        gates = g_ref[at, :]
        sums = jnp.dot(tril, gates, precision=HIGHEST, preferred_element_type=jnp.float32)
        chains = []
        for h in range(heads):
            lanes = slice(h * width, (h + 1) * width)
            k, q = k_ref[at, lanes], q_ref[at, lanes]
            v = v_ref[at, lanes].astype(jnp.float32)
            kf, qf = k.astype(jnp.float32), q.astype(jnp.float32)
            ik = lax.rsqrt(jnp.sum(kf * kf, axis=-1, keepdims=True) + TINY_NORM)
            iq = lax.rsqrt(jnp.sum(qf * qf, axis=-1, keepdims=True) + TINY_NORM)
            iq = iq * width ** (-0.5)
            beta = gates[:, h : h + 1]
            log_sum = sums[:, heads + h : heads + h + 1]
            log_full = jnp.broadcast_to(log_sum, (BLOCK, BLOCK))
            spread = log_full - log_full.T
            damp = jnp.where(causal, jnp.exp(jnp.where(causal, spread, 0.0)), 0.0)
            damp = damp * jnp.broadcast_to(ik, (BLOCK, BLOCK)).T
            lower = jnp.where(strict, nt(k, k) * damp * (beta * ik), 0.0)
            score_s[h, at, :] = (nt(q, k) * damp * iq).astype(jnp.bfloat16)
            grow = jnp.exp(log_sum)
            right = jnp.concatenate([v * beta, kf * (beta * ik * grow)], axis=1)
            tail = log_full[BLOCK - 1 : BLOCK, :]
            weighted = kf * (ik * jnp.exp(tail[:, :1] - log_sum))
            wt_s[h, c] = weighted.T.astype(jnp.bfloat16)
            tail_s[h, c] = jnp.broadcast_to(jnp.exp(tail), (8, BLOCK))
            lhs_s[h, c, BLOCK:, :] = (qf * (iq * grow)).astype(jnp.bfloat16)
            chains.append([h, lower, right, eye - jnp.where(differ == 1, lower, 0.0)])
        return at, c, chains

    def pair(p, carry):
        prepared = [prepare(p * TOGETHER + i) for i in range(TOGETHER)]
        size = 2
        while size < BLOCK:
            level = (differ >= size) & (differ < 2 * size)
            parts = [
                [mm(jnp.where(level, ch[1], 0.0), ch[3]) for ch in item[2]] for item in prepared
            ]
            for item, part in zip(prepared, parts):
                for ch, moved in zip(item[2], part):
                    ch[3] = ch[3] - mm(ch[3], moved)
            size *= 2
        for at, c, chains in prepared:
            for h, lower, right, inverse in chains:
                solved = mm(inverse, right)
                corr_s[h, at, :] = solved[:, :width]
                lhs_s[h, c, :BLOCK, :] = solved[:, width:].astype(jnp.bfloat16)
        return carry

    lax.fori_loop(0, blocks // TOGETHER, pair, 0)
    for h in range(heads):
        state_ref[h] = jnp.concatenate([eye, jnp.zeros((width, width), jnp.float32)], axis=1)

    def advance(c, carry):
        at = pl.ds(pl.multiple_of(c * BLOCK, BLOCK), BLOCK)
        boths = [mm(lhs_s[h, c], state_ref[h]) for h in range(heads)]
        fresh = []
        for h in range(heads):
            first = boths[h][:BLOCK]
            fresh.append(
                jnp.concatenate(
                    [-first[:, :width], corr_s[h, at, :] - first[:, width:]], axis=1
                ).astype(jnp.bfloat16)
            )
        for h in range(heads):
            decay = tail_s[h, c][:1, :]
            decay = jnp.concatenate([decay, decay], axis=1)
            state_ref[h] = state_ref[h] * decay + mm(wt_s[h, c], fresh[h])
        for h in range(heads):
            out = boths[h][BLOCK:] + mm(score_s[h, at, :], fresh[h])
            outa_ref[h, at, :] = out[:, :width].astype(jnp.bfloat16)
            outb_ref[h, at, :] = out[:, width:]
        return carry

    lax.fori_loop(0, blocks, advance, 0)
    final_ref[...] = state_ref[...].astype(jnp.bfloat16)


def delta_rule(query_raw, key_raw, value_raw, gates, heads, width):
    rows = query_raw.shape[0]
    blocks = rows // BLOCK
    vm = pl.BlockSpec(memory_space=pltpu.VMEM)
    return pl.pallas_call(
        functools.partial(delta_kernel, heads, width),
        out_shape=(
            jax.ShapeDtypeStruct((heads, rows, width), jnp.bfloat16),
            jax.ShapeDtypeStruct((heads, rows, width), jnp.float32),
            jax.ShapeDtypeStruct((heads, width, 2 * width), jnp.bfloat16),
        ),
        in_specs=[vm] * 4,
        out_specs=(vm, vm, vm),
        scratch_shapes=[
            pltpu.VMEM((heads, blocks, 2 * BLOCK, width), jnp.bfloat16),
            pltpu.VMEM((heads, rows, width), jnp.float32),
            pltpu.VMEM((heads, rows, BLOCK), jnp.bfloat16),
            pltpu.VMEM((heads, blocks, width, BLOCK), jnp.bfloat16),
            pltpu.VMEM((heads, blocks, 8, BLOCK), jnp.float32),
            pltpu.VMEM((heads, width, 2 * width), jnp.float32),
        ],
        compiler_params=pltpu.CompilerParams(
            vmem_limit_bytes=40 * 1024 * 1024
        ),
        cost_estimate=pl.CostEstimate(
            flops=10_000_000_000, bytes_accessed=4_000_000, transcendentals=0
        ),
        name="delta_rule",
    )(query_raw, key_raw, value_raw, gates)


MESH = pl.DeviceIdType.MESH


def sharded_place():
    tp = lax.axis_size("tp")
    me = lax.axis_index("tp")
    core = lax.rem(me, 2)
    return tp // 2, me, core, me // 2, me + 1 - 2 * core


def greet(chips, core, chip, sibling):
    barrier = pltpu.get_barrier_semaphore()
    pl.semaphore_signal(barrier, inc=1, device_id={"tp": sibling}, device_id_type=MESH)
    for o in range(1, chips):
        there = lax.rem(chip + o, chips) * 2 + core
        pl.semaphore_signal(barrier, inc=1, device_id={"tp": there}, device_id_type=MESH)
    pl.semaphore_wait(barrier, chips)


def project_kernel(heads, *refs):
    count = 7
    tok_ref, far_refs, wg_ref, rate_ref = refs[0], refs[1 : 1 + count], refs[8], refs[9]
    out_refs, gates_ref = refs[10 : 10 + count], refs[17]
    full, y_send, y_recv, own_send, own_recv, fwd_send, fwd_recv, w_sem = refs[18:26]
    w_refs = refs[26:]
    rows, part = tok_ref.shape
    step = rows // CHUNKS
    chips, me, core, chip, sibling = sharded_place()

    def columns(owner):
        return pl.ds(pl.multiple_of(owner * part, part), part)

    def at(r):
        return pl.ds(pl.multiple_of(r * step, step), step)

    def across(o, r):
        there = lax.rem(chip + o, chips) * 2 + core
        return pltpu.make_async_remote_copy(
            src_ref=tok_ref.at[at(r), :],
            dst_ref=full.at[at(r), columns(me)],
            send_sem=y_send.at[o - 1, r],
            recv_sem=y_recv.at[o - 1, r],
            device_id={"tp": there},
            device_id_type=MESH,
        )

    def beside(r):
        return pltpu.make_async_remote_copy(
            src_ref=tok_ref.at[at(r), :],
            dst_ref=full.at[at(r), columns(me)],
            send_sem=own_send.at[r],
            recv_sem=own_recv.at[r],
            device_id={"tp": sibling},
            device_id_type=MESH,
        )

    def forward(o, r):
        owner = lax.rem(chip - o + chips, chips) * 2 + core
        block = full.at[at(r), columns(owner)]
        return pltpu.make_async_remote_copy(
            src_ref=block,
            dst_ref=block,
            send_sem=fwd_send.at[o - 1, r],
            recv_sem=fwd_recv.at[o - 1, r],
            device_id={"tp": sibling},
            device_id_type=MESH,
        )

    greet(chips, core, chip, sibling)
    for r in range(CHUNKS):
        for o in range(1, chips):
            across(o, r).start()
    loads = [
        pltpu.make_async_copy(far, w_ref, w_sem.at[i])
        for i, (far, w_ref) in enumerate(zip(far_refs, w_refs))
    ]
    for load in loads:
        load.start()
    for r in range(CHUNKS):
        beside(r).start()
    full[:, columns(me)] = tok_ref[...]

    def chunk(first, pieces, carry):
        for i in range(pieces):
            for o in range(1, chips):
                across(o, first + i).wait_recv()
                forward(o, first + i).start()
        for i in range(pieces):
            beside(first + i).wait_recv()
            for o in range(1, chips):
                forward(o, first + i).wait_recv()
        size = step * pieces
        here = pl.ds(pl.multiple_of(first * step, step), size)
        squares = jnp.zeros((size, 1), jnp.float32)
        for b in range(2 * chips):
            piece = full[here, b * part : (b + 1) * part].astype(jnp.float32)
            squares = squares + jnp.sum(piece * piece, axis=1, keepdims=True)
        inv_rms = lax.rsqrt(squares / (part * 2 * chips) + TINY_NORM)
        for w_ref, out_ref in zip(w_refs, out_refs):
            summed = jnp.dot(full[here, :], w_ref[...], preferred_element_type=jnp.float32)
            out_ref[here, :] = (summed * inv_rms).astype(jnp.bfloat16)
        raw = jnp.dot(full[here, :], wg_ref[...], preferred_element_type=jnp.float32) * inv_rms
        lane = lax.broadcasted_iota(jnp.int32, raw.shape, 1)
        softplus = jnp.maximum(raw, 0.0) + jnp.log1p(jnp.exp(-jnp.abs(raw)))
        gates_ref[here, :] = jnp.where(lane < heads, jax.nn.sigmoid(raw), -rate_ref[...] * softplus)
        return carry

    for load in loads:
        load.wait()
    paired = CHUNKS // 2 - 1
    lax.fori_loop(0, paired, lambda r, carry: chunk(2 * r, 2, carry), 0)
    lax.fori_loop(2 * paired, CHUNKS, lambda r, carry: chunk(r, 1, carry), 0)
    for r in range(CHUNKS):
        for o in range(1, chips):
            across(o, r).wait_send()
            forward(o, r).wait_send()
        beside(r).wait_send()


def project(tokens, weights, w_gates, rates, heads):
    rows, part = tokens.shape
    tp = lax.axis_size("tp")
    others = max(tp // 2 - 1, 1)
    vm = pl.BlockSpec(memory_space=pltpu.VMEM)
    dma = pltpu.SemaphoreType.DMA
    return pl.pallas_call(
        functools.partial(project_kernel, heads),
        out_shape=tuple(
            jax.ShapeDtypeStruct((rows, w.shape[1]), jnp.bfloat16) for w in weights
        )
        + (jax.ShapeDtypeStruct((rows, w_gates.shape[1]), jnp.float32),),
        in_specs=[vm] + [pl.BlockSpec(memory_space=pl.ANY)] * len(weights) + [vm] * 2,
        out_specs=(vm,) * (1 + len(weights)),
        scratch_shapes=[
            pltpu.VMEM((rows, part * tp), jnp.bfloat16),
            dma((others, CHUNKS)),
            dma((others, CHUNKS)),
            dma((CHUNKS,)),
            dma((CHUNKS,)),
            dma((others, CHUNKS)),
            dma((others, CHUNKS)),
            dma((len(weights),)),
        ]
        + [pltpu.VMEM(w.shape, w.dtype) for w in weights],
        compiler_params=pltpu.CompilerParams(
            collective_id=0, has_side_effects=True, vmem_limit_bytes=48 * 1024 * 1024
        ),
        cost_estimate=pl.CostEstimate(
            flops=10_000_000_000, bytes_accessed=20_000_000, transcendentals=0
        ),
        name="gather_project",
    )(tokens, *weights, w_gates, rates)


def middle_kernel(
    heads, width, final_ref, gv_ref, gg_ref, cg_ref, taps_ref, ln_gain_ref, ln_shift_ref,
    outa_ref, outb_ref, dg_ref, gain_ref, mixed_ref, conv_ref,
    padded, filtered, halo_out, halo_in, sums_out, sums_in, near, window_s, sent_s, far_s,
    near_send, near_recv, far_send, far_recv, halo_send, halo_recv, ln_send, ln_recv,
):
    rows = gv_ref.shape[0]
    halo = halo_in.shape[0]
    lanes = padded.shape[2]
    groups = padded.shape[0]
    kernel = taps_ref.shape[0]
    tiles = rows // BLOCK
    sp, place = lax.axis_size("sp"), lax.axis_index("sp")
    tp, me = lax.axis_size("tp"), lax.axis_index("tp")
    reaches = [2]
    while 2 * reaches[-1] < sp:
        reaches.append(2 * reaches[-1])
    distances = [1, 2] + reaches[1:]
    barrier = pltpu.get_barrier_semaphore()
    for step in distances:
        for to in (step, sp - step):
            pl.semaphore_signal(
                barrier, inc=1, device_id={"sp": lax.rem(place + to, sp)}, device_id_type=MESH
            )
    for step in range(1, tp):
        pl.semaphore_signal(
            barrier, inc=1, device_id={"tp": lax.rem(me + step, tp)}, device_id_type=MESH
        )
    pl.semaphore_wait(barrier, 2 * len(distances) + tp - 1)

    def onward(src, dst, send, recv, step):
        return pltpu.make_async_remote_copy(
            src_ref=src,
            dst_ref=dst,
            send_sem=send,
            recv_sem=recv,
            device_id={"sp": lax.rem(place + step, sp)},
            device_id_type=MESH,
        )

    firsts = [
        onward(final_ref, near.at[i], near_send.at[i], near_recv.at[i], i + 1) for i in range(2)
    ]
    for copy in firsts:
        copy.start()

    def at(t):
        return pl.ds(pl.multiple_of(t * BLOCK, BLOCK), BLOCK)

    def unit(t, carry):
        value = gv_ref[at(t), :].astype(jnp.float32)
        units = (value * jax.nn.sigmoid(gg_ref[at(t), :].astype(jnp.float32))).astype(jnp.bfloat16)
        wide = units.astype(jnp.float32)
        for g in range(groups):
            padded[g, pl.ds(pl.multiple_of(t * BLOCK + halo, halo), BLOCK), :] = wide[
                :, g * lanes : (g + 1) * lanes
            ]
        return units

    units = unit(tiles - 1, 0)
    halo_out[...] = units[BLOCK - halo :, :]
    halo_copy = onward(halo_out, halo_in, halo_send.at[0], halo_recv.at[0], 1)
    halo_copy.start()

    def unit_loop(t, carry):
        unit(t, 0)
        return carry

    lax.fori_loop(0, tiles - 1, unit_loop, 0)

    def conv(t, carry):
        first = jnp.zeros((BLOCK, 1), jnp.float32)
        second = jnp.zeros((BLOCK, 1), jnp.float32)
        for g in range(groups):
            total = jnp.zeros((BLOCK, lanes), jnp.float32)
            for j in range(kernel):
                start = t * BLOCK + (halo - kernel + 1 + j)
                tap = taps_ref[j : j + 1, g * lanes : (g + 1) * lanes]
                total = total + padded[g, pl.ds(start, BLOCK), :] * tap
            filtered[g, at(t), :] = total
            first = first + jnp.sum(total, axis=1, keepdims=True)
            second = second + jnp.sum(total * total, axis=1, keepdims=True)
        lane = lax.broadcasted_iota(jnp.int32, (BLOCK, BLOCK), 1)
        sums_out[t] = jnp.where(lane == 0, first, jnp.where(lane == 1, second, 0.0)).T[:8, :]
        return carry

    half = tiles // 2
    lax.fori_loop(1, half, conv, 0)
    for copy in firsts:
        copy.wait()
    for h in range(heads):
        one = jnp.where(place >= 1, near[0, h].astype(jnp.float32), 0.0)
        two = jnp.where(place >= 2, near[1, h].astype(jnp.float32), 0.0)
        moved = mm(one[:, :width], two)
        window_s[h] = jnp.concatenate(
            [moved[:, :width], moved[:, width:] + one[:, width:]], axis=1
        )
        sent_s[0, h] = window_s[h].astype(jnp.bfloat16)

    def step_copy(i):
        return onward(sent_s.at[i], far_s.at[i], far_send.at[i], far_recv.at[i], reaches[i])

    step_copy(0).start()
    lax.fori_loop(half, tiles, conv, 0)
    halo_copy.wait()
    before = jnp.where(place >= 1, halo_in[...].astype(jnp.float32), 0.0)
    for g in range(groups):
        padded[g, :halo, :] = before[:, g * lanes : (g + 1) * lanes]
    conv(0, 0)

    def ln_copy(step):
        return pltpu.make_async_remote_copy(
            src_ref=sums_out,
            dst_ref=sums_in.at[step - 1],
            send_sem=ln_send.at[step - 1],
            recv_sem=ln_recv.at[step - 1],
            device_id={"tp": lax.rem(me + step, tp)},
            device_id_type=MESH,
        )

    for step in range(1, tp):
        ln_copy(step).start()
    for i in range(len(reaches) - 1):
        step_copy(i).wait()
        for h in range(heads):
            earlier = jnp.where(place >= reaches[i], far_s[i, h].astype(jnp.float32), 0.0)
            window = window_s[h]
            moved = mm(window[:, :width], earlier)
            window_s[h] = jnp.concatenate(
                [moved[:, :width], moved[:, width:] + window[:, width:]], axis=1
            )
            sent_s[i + 1, h] = window_s[h].astype(jnp.bfloat16)
        step_copy(i + 1).start()
    for step in range(1, tp):
        ln_copy(step).wait()
    channels = groups * lanes * tp

    def norm(t, carry):
        sums = sums_out[t]
        for step in range(1, tp):
            sums = sums + sums_in[step - 1, t]
        sums = jnp.concatenate([sums, jnp.zeros((BLOCK - 8, BLOCK), jnp.float32)], axis=0).T
        center = sums[:, 0:1] / channels
        variance = jnp.maximum(sums[:, 1:2] / channels - center * center, 0.0)
        scale = lax.rsqrt(variance + TINY_VAR)
        for g in range(groups):
            cut = slice(g * lanes, (g + 1) * lanes)
            normed = (filtered[g, at(t), :] - center) * scale
            normed = normed * ln_gain_ref[:, cut] + ln_shift_ref[:, cut]
            gate = cg_ref[at(t), cut].astype(jnp.float32)
            conv_ref[at(t), cut] = (jax.nn.silu(normed) * jax.nn.silu(gate)).astype(jnp.bfloat16)
        return carry

    lax.fori_loop(0, tiles, norm, 0)
    last = len(reaches) - 1
    step_copy(last).wait()
    carried = []
    for h in range(heads):
        earlier = jnp.where(
            place >= reaches[last], far_s[last, h, :, width:].astype(jnp.float32), 0.0
        )
        window = window_s[h]
        carried.append((mm(window[:, :width], earlier) + window[:, width:]).astype(jnp.bfloat16))

    def one_tile(t, carry):
        for h in range(heads):
            cut = slice(h * width, (h + 1) * width)
            result = outb_ref[h, at(t), :] + mm(outa_ref[h, at(t), :], carried[h])
            result = result * lax.rsqrt(
                jnp.mean(result * result, axis=-1, keepdims=True) + TINY_NORM
            )
            gate = dg_ref[at(t), cut].astype(jnp.float32)
            mixed_ref[at(t), cut] = (result * gain_ref[...] * jax.nn.silu(gate)).astype(
                jnp.bfloat16
            )
        return carry

    lax.fori_loop(0, tiles, one_tile, 0)


def middle(final, glu_value, glu_gate, conv_gate, taps, ln_gain, ln_shift, outa, outb, gate, gain):
    heads, width = final.shape[0], final.shape[1]
    rows, channels = glu_value.shape
    kernel = taps.shape[0]
    halo = (kernel - 1 + 31) // 32 * 32
    lanes = min(channels, 128)
    groups = channels // lanes
    sp, tp = lax.axis_size("sp"), lax.axis_size("tp")
    steps = 1
    while 2 ** (steps + 1) < sp:
        steps += 1
    vm = pl.BlockSpec(memory_space=pltpu.VMEM)
    dma = pltpu.SemaphoreType.DMA
    tiles = rows // BLOCK
    pair = (heads, width, 2 * width)
    return pl.pallas_call(
        functools.partial(middle_kernel, heads, width),
        out_shape=(
            jax.ShapeDtypeStruct((rows, heads * width), jnp.bfloat16),
            jax.ShapeDtypeStruct((rows, channels), jnp.bfloat16),
        ),
        in_specs=[vm] * 11,
        out_specs=(vm, vm),
        scratch_shapes=[
            pltpu.VMEM((groups, halo + rows, lanes), jnp.float32),
            pltpu.VMEM((groups, rows, lanes), jnp.float32),
            pltpu.VMEM((halo, channels), jnp.bfloat16),
            pltpu.VMEM((halo, channels), jnp.bfloat16),
            pltpu.VMEM((tiles, 8, BLOCK), jnp.float32),
            pltpu.VMEM((tp - 1, tiles, 8, BLOCK), jnp.float32),
            pltpu.VMEM((2,) + pair, jnp.bfloat16),
            pltpu.VMEM(pair, jnp.float32),
            pltpu.VMEM((steps,) + pair, jnp.bfloat16),
            pltpu.VMEM((steps,) + pair, jnp.bfloat16),
            dma((2,)),
            dma((2,)),
            dma((steps,)),
            dma((steps,)),
            dma((1,)),
            dma((1,)),
            dma((tp - 1,)),
            dma((tp - 1,)),
        ],
        compiler_params=pltpu.CompilerParams(
            collective_id=2, has_side_effects=True, vmem_limit_bytes=40 * 1024 * 1024
        ),
        cost_estimate=pl.CostEstimate(
            flops=10_000_000_000, bytes_accessed=20_000_000, transcendentals=0
        ),
        name="exchange_middle",
    )(final, glu_value, glu_gate, conv_gate, taps, ln_gain, ln_shift, outa, outb, gate, gain)


def output_kernel(
    dm_ref, cm_ref, wd_ref, wc_ref, out_ref,
    beside_out, beside_in, across_out, across_in, b_send, b_recv, y_send, y_recv,
):
    chips, me, core, chip, sibling = sharded_place()
    rows = out_ref.shape[0]
    width = out_ref.shape[1] // CUTS

    def cols(n):
        return pl.ds(pl.multiple_of(n * width, width), width)

    def partial(target, n):
        at = pl.ds(pl.multiple_of(target * rows, rows), rows)
        summed = jnp.dot(dm_ref[at, :], wd_ref[:, cols(n)], preferred_element_type=jnp.float32)
        return summed + jnp.dot(
            cm_ref[at, :], wc_ref[:, cols(n)], preferred_element_type=jnp.float32
        )

    def beside(o, n):
        return pltpu.make_async_remote_copy(
            src_ref=beside_out.at[o, n],
            dst_ref=beside_in.at[o, n],
            send_sem=b_send.at[o, n],
            recv_sem=b_recv.at[o, n],
            device_id={"tp": sibling},
            device_id_type=MESH,
        )

    def across(o, n):
        there = lax.rem(chip + o, chips) * 2 + core
        return pltpu.make_async_remote_copy(
            src_ref=across_out.at[o - 1, n],
            dst_ref=across_in.at[o - 1, n],
            send_sem=y_send.at[o - 1, n],
            recv_sem=y_recv.at[o - 1, n],
            device_id={"tp": there},
            device_id_type=MESH,
        )

    greet(chips, core, chip, sibling)
    order = list(range(1, chips)) + [0]
    for o in order:
        their_chip = lax.rem(chip + o, chips) * 2

        def give(n, carry, o=o, their_chip=their_chip):
            beside_out[o, n] = partial(their_chip + 1 - core, n).astype(jnp.bfloat16)
            beside(o, n).start()
            return carry

        def keep(n, carry, o=o, their_chip=their_chip):
            mine = partial(their_chip + core, n)
            beside(o, n).wait_recv()
            mine = mine + beside_in[o, n].astype(jnp.float32)
            across_out[o - 1, n] = mine.astype(jnp.bfloat16)
            across(o, n).start()
            return carry

        if o != 0:

            def both(n, carry, give=give, keep=keep):
                @pl.when(n + 1 < CUTS)
                def _():
                    give(n + 1, 0)

                return keep(n, carry)

            give(0, 0)
            lax.fori_loop(0, CUTS, both, 0)
        else:
            lax.fori_loop(0, CUTS, give, 0)

    def close(n, carry):
        mine = partial(me, n)
        beside(0, n).wait_recv()
        mine = mine + beside_in[0, n].astype(jnp.float32)
        for o in range(1, chips):
            across(o, n).wait_recv()
            mine = mine + across_in[o - 1, n].astype(jnp.float32)
        out_ref[:, cols(n)] = mine.astype(jnp.bfloat16)
        return carry

    lax.fori_loop(0, CUTS, close, 0)

    def drain(n, carry):
        for o in range(chips):
            beside(o, n).wait_send()
        for o in range(1, chips):
            across(o, n).wait_send()
        return carry

    lax.fori_loop(0, CUTS, drain, 0)


def output_projection(delta_mixed, conv_mixed, out_delta, out_conv):
    tp = lax.axis_size("tp")
    chips = tp // 2
    others = max(chips - 1, 1)
    rows = delta_mixed.shape[0] // tp
    width = out_delta.shape[1]
    cut = width // CUTS
    vm = pl.BlockSpec(memory_space=pltpu.VMEM)
    dma = pltpu.SemaphoreType.DMA
    return pl.pallas_call(
        output_kernel,
        out_shape=jax.ShapeDtypeStruct((rows, width), jnp.bfloat16),
        in_specs=[vm] * 4,
        out_specs=vm,
        scratch_shapes=[
            pltpu.VMEM((chips, CUTS, rows, cut), jnp.bfloat16),
            pltpu.VMEM((chips, CUTS, rows, cut), jnp.bfloat16),
            pltpu.VMEM((others, CUTS, rows, cut), jnp.bfloat16),
            pltpu.VMEM((others, CUTS, rows, cut), jnp.bfloat16),
            dma((chips, CUTS)),
            dma((chips, CUTS)),
            dma((others, CUTS)),
            dma((others, CUTS)),
        ],
        compiler_params=pltpu.CompilerParams(
            collective_id=1, has_side_effects=True, vmem_limit_bytes=48 * 1024 * 1024
        ),
        cost_estimate=pl.CostEstimate(
            flops=10_000_000_000, bytes_accessed=20_000_000, transcendentals=0
        ),
        name="output_scatter",
    )(delta_mixed, conv_mixed, out_delta, out_conv)


def local(
    tokens,
    w_query,
    w_key,
    w_value,
    w_delta_gate,
    w_glu_value,
    w_glu_gate,
    w_conv_gate,
    w_beta,
    w_decay,
    decay_log,
    head_gain,
    conv_taps,
    ln_gain,
    ln_shift,
    out_delta,
    out_conv,
):
    head_size = head_gain.shape[0]
    heads_here = w_query.shape[1] // head_size
    first_head = lax.axis_index("tp") * heads_here
    rates = jnp.exp(lax.dynamic_slice_in_dim(decay_log, first_head, heads_here, 0))
    fill = head_size - 2 * heads_here
    rates = jnp.concatenate(
        [jnp.zeros((heads_here,), jnp.float32), rates, jnp.zeros((fill,), jnp.float32)]
    )[None, :]
    w_gates = jnp.concatenate(
        [
            lax.dynamic_slice_in_dim(w_beta, first_head, heads_here, 1),
            lax.dynamic_slice_in_dim(w_decay, first_head, heads_here, 1),
            jnp.zeros((w_beta.shape[0], fill), jnp.bfloat16),
        ],
        axis=1,
    )
    weights = (w_query, w_key, w_value, w_delta_gate, w_glu_value, w_glu_gate, w_conv_gate)
    (
        query_raw,
        key_raw,
        value_raw,
        delta_gate_raw,
        glu_value_raw,
        glu_gate_raw,
        conv_gate_raw,
        gates,
    ) = project(tokens, weights, w_gates, rates, heads_here)
    outa, outb, final = delta_rule(
        query_raw, key_raw, value_raw, gates, heads_here, head_size
    )
    delta_mixed, conv_mixed = middle(
        final,
        glu_value_raw,
        glu_gate_raw,
        conv_gate_raw,
        conv_taps.astype(jnp.float32),
        ln_gain[None, :],
        ln_shift[None, :],
        outa,
        outb,
        delta_gate_raw,
        head_gain[None, :],
    )
    return output_projection(delta_mixed, conv_mixed, out_delta, out_conv)


def solution(mesh):
    return jax.shard_map(
        local,
        mesh=mesh,
        in_specs=(
            P("sp", "tp"),
            P(None, "tp"),
            P(None, "tp"),
            P(None, "tp"),
            P(None, "tp"),
            P(None, "tp"),
            P(None, "tp"),
            P(None, "tp"),
            P(),
            P(),
            P(),
            P(),
            P(None, "tp"),
            P("tp"),
            P("tp"),
            P("tp", None),
            P("tp", None),
        ),
        out_specs=P(("sp", "tp"), None),
        check_vma=False,
    )
```
